128 devices in a mesh: sp: 64 (over z, y, x), tp: 2 (over core).
Axes of the slice: x: 4, y: 4, z: 4, core: 2. Of those that a mesh axis runs over, the one named last changes fastest.
Arguments:
- queries: bfloat16 [16384, 1024], P('sp', 'tp'), may hold values from -6 to 6
- keys: bfloat16 [16384, 256], P('sp', 'tp'), may hold values from -6 to 6
- values: bfloat16 [16384, 256], P('sp', 'tp'), may hold values from -24 to 24
- sink_logit: float32 [16], P('tp'), may hold values from 3 to 7
- w_out: bfloat16 [1024, 2048], replicated, may hold values from -0.1875 to 0.1875
- residual: bfloat16 [16384, 2048], P(('sp', 'tp')), may hold values from -3 to 3
- norm_gain: float32 [2048], replicated, may hold values from 0.1 to 1.9
- w_gate: bfloat16 [64, 2048, 2048], P('sp', None, 'tp'), may hold values from -0.5 to 0.5
- w_up: bfloat16 [64, 2048, 2048], P('sp', None, 'tp'), may hold values from -0.5 to 0.5
- w_down: bfloat16 [64, 2048, 2048], P('sp', 'tp'), may hold values from -0.125 to 0.125
- expert_ids: int32 [16384, 2], P(('sp', 'tp')), may hold values from 0 to 63, all different within a row; in each aligned block of 128 rows (0 to 127, 128 to 255, ...) at most 6 rows name the same one
- route_weight: float32 [16384, 2], P(('sp', 'tp')), may hold values from 0.2 to 1
Outputs:
- final: bfloat16 [16384, 2048], P(('sp', 'tp'))
The draws below stay inside these ranges and needn't reach their ends.
Inputs may be any that keep to these rules, and one draw needn't show every extreme that they name: `expert_ids`: in the rows of one device each row names 2 different experts and no expert is named by more than 6 rows; some expert is named by exactly 6 of them.
All inputs are finite; a program needn't handle non-finite values.
Results may differ from the reference program's by a relative error of at most 0.0097.
Values may be sent and summed in bfloat16 or wider, within the bound.
A program may use at most 128 MiB of HBM per device.

```python
import math
import jax
import jax.numpy as jnp
import numpy as np
from jax import lax

D = 2048
HEADS = 16
KV_HEADS = 4
HEAD_DIM = 64
FF = 2048
WINDOW = 128
TOPK = 2
SPAN = 256
EXPERTS = 64
CAP = 6
SEQ = 16384
N_TP = 2


def draw_queries(key, part):
    noise_draw = jnp.clip(jax.random.normal(jax.random.fold_in(key, 1), (SEQ, KV_HEADS, HEADS // KV_HEADS, HEAD_DIM), jnp.float32), -4.0, 4.0)
    return noise_draw.reshape(SEQ, HEADS * HEAD_DIM).astype(jnp.bfloat16)


def draw_keys(key, part):
    noise_draw = jnp.clip(jax.random.normal(jax.random.fold_in(key, 2), (SEQ, KV_HEADS, 1, HEAD_DIM), jnp.float32), -4.0, 4.0)
    return noise_draw.reshape(SEQ, KV_HEADS * HEAD_DIM).astype(jnp.bfloat16)


def expert_matrix(key):
    weight_scale = D ** (-0.5)
    drawn = weight_scale * jax.random.normal(key, (EXPERTS, D, FF), jnp.float32)
    return jnp.clip(drawn, -0.5, 0.5).astype(jnp.bfloat16)


def draw_w_gate(key, part):
    return expert_matrix(jax.random.fold_in(key, 11))


def draw_w_up(key, part):
    return expert_matrix(jax.random.fold_in(key, 13))


def levels(rng, dims, cuts, least, largest):
    level = 1.0
    for axis_at, shards_of in cuts:
        steps = jax.random.uniform(jax.random.fold_in(jax.random.fold_in(rng, 6), axis_at), (shards_of,), jnp.float32, least / len(cuts), largest / len(cuts))
        level = level * jnp.repeat(jnp.exp(steps), dims[axis_at] // shards_of).reshape((-1,) + (1,) * (len(dims) - 1 - axis_at))
    return level


def deal_out(stream_key, own, number, rows, number_of, top, bound, lean):
    sequence = jax.random.permutation(stream_key, number_of)
    packed, usual = load_shares(number_of, rows * top, bound, lean, True), load_shares(number_of, rows * top, bound, lean, False)
    places = jnp.arange(number_of)

    def named(sizes, rotation):
        used = int((sizes > 0).sum())
        fixed = max(1, used // 4)
        shifted = fixed + (places - fixed + rotation * (used - fixed)) % max(1, number_of - fixed)
        return jnp.zeros((number_of,), jnp.int32).at[sequence[jnp.where(places < fixed, places, shifted)]].set(jnp.asarray(sizes, jnp.int32))

    sizes = jnp.where(number % 4 == 0, named(packed, number // 4), named(usual, number - number // 4 - 1))
    mixed = jax.random.permutation(jax.random.fold_in(own, 3), number_of)
    source_of, taker = mixed[0:number_of // 2 * 2:2], mixed[1:number_of // 2 * 2:2]
    margin = jnp.minimum(sizes[source_of] - 1, bound - sizes[taker]) // 2
    margin = jnp.where((source_of == sequence[0]) | (taker == sequence[0]) | (sizes[taker] == 0), 0, jnp.maximum(margin, 0))
    shifted = jax.random.randint(jax.random.fold_in(own, 4), (number_of // 2,), 0, 1 << 20) % (margin + 1)
    sizes = sizes.at[source_of].add(-shifted).at[taker].add(shifted)
    items = jnp.searchsorted(jnp.cumsum(sizes), jnp.arange(rows * top), side="right").astype(jnp.int32)
    table = items.reshape(top, rows).T
    table = table[jax.random.permutation(jax.random.fold_in(own, 1), rows)]
    rotation = jax.random.randint(jax.random.fold_in(own, 2), (rows, 1), 0, top)
    return jnp.take_along_axis(table, (jnp.arange(top)[None, :] + rotation) % top, axis=1)


def load_shares(number_of, total, reach, slope, full):
    portions = [(1 << 20) // math.isqrt(rank ** slope) + 1 for rank in range(1, number_of + 1)]
    largest = reach if full else min(reach, max(-(-total // number_of), total * portions[0] // sum(portions)))
    least = 1 if total - largest >= number_of - 1 else 0
    holding, surplus = [largest] + [least] * (number_of - 1), total - largest - least * (number_of - 1)
    while surplus > 0:
        movable = [i for i in range(1, number_of) if holding[i] < largest] or [i for i in range(1, number_of) if holding[i] < reach]
        mass, left = sum([portions[i] for i in movable]), surplus
        for i in movable:
            extra = min(reach - holding[i], max(1, left * portions[i] // mass), surplus)
            holding[i] = holding[i] + extra
            surplus = surplus - extra
    return np.array(holding)


def normal_values(key, dims, spread, reach, shards=(), kind=jnp.bfloat16):
    level = levels(key, dims, shards, -0.22, 0.18) if shards else 1.0
    array = jax.random.normal(key, dims, jnp.float32) * spread * level
    return jnp.minimum(jnp.maximum(array, -reach), reach).astype(kind)


def setup_inputs(seed: int = 0) -> dict:
    splits = jax.random.split(jax.random.key(seed), 13)
    queries = draw_queries(jax.random.fold_in(splits[12], 71), 0)
    keys = draw_keys(jax.random.fold_in(splits[12], 71), 0)
    values = normal_values(splits[2], (SEQ, KV_HEADS * HEAD_DIM), 4.0, 24.0, ((0, 64), (1, 2)))
    sink_logit = jnp.clip(3.0 + 4.0 * jax.random.uniform(splits[3], (HEADS,), jnp.float32) ** levels(splits[3], (HEADS,), ((0, 2),), -0.2, 0.2), 3.0, 7.0)
    w_out = normal_values(splits[4], (HEADS * HEAD_DIM, D), (HEADS * HEAD_DIM) ** -0.5, 0.1875)
    residual = normal_values(splits[5], (SEQ, D), 0.5, 3.0, ((0, 128),))
    norm_gain = jnp.clip(1.0 + 0.18 * jax.random.normal(splits[6], (D,), jnp.float32), 0.1, 1.9)
    w_gate = draw_w_gate(jax.random.fold_in(splits[12], 71), 0)
    w_up = draw_w_up(jax.random.fold_in(splits[12], 71), 0)
    w_down = normal_values(splits[9], (EXPERTS, FF, D), FF ** -0.5, 0.125, ((0, 64), (1, 2)))
    expert_ids_keys = jax.random.split(jax.random.fold_in(splits[10], 1), SEQ // (SPAN // N_TP))
    expert_ids_turns = jax.random.permutation(jax.random.fold_in(splits[10], 3), SEQ // (SPAN // N_TP))
    expert_ids = jax.vmap(lambda own, number: deal_out(jax.random.fold_in(splits[10], 2), own, number, SPAN // N_TP, EXPERTS, TOPK, CAP, 2))(expert_ids_keys, expert_ids_turns).reshape((SEQ, TOPK))
    route_weight = jnp.clip(0.2 + 0.8 * jax.random.uniform(splits[11], (SEQ, TOPK), jnp.float32) ** levels(splits[11], (SEQ, TOPK), ((0, 128),), -0.2, 0.2), 0.2, 1.0)
    return dict(queries=queries, keys=keys, values=values, sink_logit=sink_logit, w_out=w_out, residual=residual, norm_gain=norm_gain, w_gate=w_gate, w_up=w_up, w_down=w_down, expert_ids=expert_ids, route_weight=route_weight)


CLAMP_LIMIT = 7.0
GATE_ALPHA = 1.702
EPSILON = 1e-06
NEG_BIG = -1e+30
SORT_ROWS = 128

def reference(queries, keys, values, sink_logit, w_out, residual, norm_gain, w_gate, w_up, w_down, expert_ids, route_weight):
    seq_len = queries.shape[0]
    repeat = HEADS // KV_HEADS
    block_count = seq_len // SPAN
    keys_pad = jnp.pad(keys, ((WINDOW, WINDOW), (0, 0))).reshape(seq_len + 2 * WINDOW, KV_HEADS, HEAD_DIM)
    values_pad = jnp.pad(values, ((WINDOW, WINDOW), (0, 0))).reshape(seq_len + 2 * WINDOW, KV_HEADS, HEAD_DIM)
    query_blocks = queries.reshape(block_count, SPAN, KV_HEADS, repeat, HEAD_DIM)
    logit_sink = sink_logit.astype(jnp.float32).reshape(KV_HEADS, repeat)[:, :, None, None]

    def attend_block(inputs):
        query_block, block_index = inputs
        row_start = block_index * SPAN
        key_block = lax.dynamic_slice_in_dim(keys_pad, row_start, SPAN + 2 * WINDOW, 0)
        value_block = lax.dynamic_slice_in_dim(values_pad, row_start, SPAN + 2 * WINDOW, 0)
        scores = jnp.einsum('qgrd,kgd->grqk', query_block.astype(jnp.float32), key_block.astype(jnp.float32)) * HEAD_DIM ** (-0.5)
        query_pos = row_start + jnp.arange(SPAN, dtype=jnp.int32)
        key_pos = row_start - WINDOW + jnp.arange(SPAN + 2 * WINDOW, dtype=jnp.int32)
        key_gap = key_pos[None, :] - query_pos[:, None]
        in_window = (jnp.abs(key_gap) <= WINDOW) & (key_pos[None, :] >= 0) & (key_pos[None, :] < seq_len)
        scores = jnp.where(in_window, scores, NEG_BIG)
        peak = jnp.maximum(lax.optimization_barrier(jnp.max(scores, axis=-1, keepdims=True)), logit_sink)
        expo = jnp.exp(scores - peak)
        divisor = lax.optimization_barrier(jnp.sum(expo, axis=-1, keepdims=True)) + jnp.exp(logit_sink - peak)
        softmax_w = (expo / divisor).astype(jnp.bfloat16)
        mixed = jnp.einsum('grqk,kgd->qgrd', softmax_w.astype(jnp.float32), value_block.astype(jnp.float32))
        return mixed.reshape(SPAN, HEADS * HEAD_DIM).astype(jnp.bfloat16)
    attended = lax.map(attend_block, (query_blocks, jnp.arange(block_count, dtype=jnp.int32)))
    attended = attended.reshape(seq_len, HEADS * HEAD_DIM)
    attn_proj = lax.optimization_barrier(jnp.dot(attended, w_out, preferred_element_type=jnp.float32).astype(jnp.bfloat16))
    midway = residual.astype(jnp.float32) + attn_proj.astype(jnp.float32)
    normed = (midway * lax.rsqrt(lax.optimization_barrier(jnp.mean(midway * midway, axis=-1, keepdims=True)) + EPSILON) * norm_gain).astype(jnp.bfloat16)
    assigned = expert_ids.reshape(-1).astype(jnp.int32)
    count_all = assigned.shape[0]
    sort_order = jnp.argsort(assigned, stable=True).astype(jnp.int32)
    sorted_expert = assigned[sort_order]
    counts = lax.optimization_barrier(jnp.sum((assigned[:, None] == jnp.arange(EXPERTS, dtype=jnp.int32)[None, :]).astype(jnp.int32), axis=0))
    filled = (counts + SORT_ROWS - 1) // SORT_ROWS * SORT_ROWS
    pad_ends = jnp.cumsum(filled).astype(jnp.int32)
    pad_starts = pad_ends - filled
    plain_starts = (jnp.cumsum(counts) - counts).astype(jnp.int32)
    slot_of = (pad_starts[sorted_expert] + jnp.arange(count_all, dtype=jnp.int32) - plain_starts[sorted_expert]).astype(jnp.int32)
    slot_total = count_all + EXPERTS * SORT_ROWS
    block_total = slot_total // SORT_ROWS
    slot_token = jnp.zeros((slot_total,), jnp.int32).at[slot_of].set(sort_order // TOPK)
    block_expert = jnp.minimum(jnp.searchsorted(pad_ends, jnp.arange(block_total, dtype=jnp.int32) * SORT_ROWS, side='right'), EXPERTS - 1).astype(jnp.int32)
    inputs = normed[slot_token].reshape(block_total, SORT_ROWS, D)
    half_width = FF // N_TP

    def expert_block(pair_in):
        rows_in, expert = pair_in
        gate_pre = jnp.dot(rows_in, w_gate[expert], preferred_element_type=jnp.float32)
        up_pre = jnp.dot(rows_in, w_up[expert], preferred_element_type=jnp.float32)
        act_clip = jnp.minimum(gate_pre, CLAMP_LIMIT)
        up_clip = jnp.clip(up_pre, -CLAMP_LIMIT, CLAMP_LIMIT)
        hidden = ((up_clip + 1.0) * act_clip * jax.nn.sigmoid(GATE_ALPHA * act_clip)).astype(jnp.bfloat16)
        down_full = w_down[expert]
        summed = jnp.zeros((rows_in.shape[0], D), jnp.float32)
        for half in range(N_TP):
            down_part = jnp.dot(hidden[:, half * half_width:(half + 1) * half_width], down_full[half * half_width:(half + 1) * half_width], preferred_element_type=jnp.float32)
            summed = summed + down_part.astype(jnp.bfloat16).astype(jnp.float32)
        return summed.astype(jnp.bfloat16)
    slot_out = lax.map(expert_block, (inputs, block_expert)).reshape(slot_total, D)
    assign_slot = jnp.zeros((count_all,), jnp.int32).at[sort_order].set(slot_of)
    picked = slot_out[assign_slot].reshape(seq_len, TOPK, D)
    routed = lax.optimization_barrier(jnp.sum(picked.astype(jnp.float32) * route_weight[:, :, None], axis=1))
    return (midway + routed).astype(jnp.bfloat16)
```

```python
import functools
import random

import jax
import jax.numpy as jnp
from jax import lax
from jax.experimental import pallas as pl
from jax.experimental.pallas import tpu as pltpu
from jax.sharding import PartitionSpec as P

MESH = pl.DeviceIdType.MESH
BF = jnp.bfloat16
F32 = jnp.float32

NSP = 64
WIN = 128
DM = 2048
HID = 1024
SLOT = 6
PAD = 8
WAVES = 4
PER = NSP // WAVES
HALF = PER * PAD
ROWS = 2 * HALF
CLAMP_LIMIT = 7.0
GATE_ALPHA = 1.702
EPSILON = 1e-06
NEG_BIG = -1e30
EXP_SCALE = 1.4426950408889634 / 8.0


def offsets():
    every = [(a, b, c) for a in range(4) for b in range(4) for c in range(4)]
    seen, groups = {(0, 0, 0)}, []
    for o in every:
        if o in seen:
            continue
        group = []
        for p in ((0, 1, 2), (1, 2, 0), (2, 0, 1)):
            for s in (1, -1):
                m = tuple((s * o[i]) % 4 for i in p)
                if m not in group:
                    group.append(m)
        seen |= set(group)
        groups.append(group)
    random.Random(1).shuffle(groups)
    groups.sort(key=lambda g: -sum(min(v, 4 - v) for v in g[0]))
    return [(0, 0, 0)] + [o for g in groups for o in g]


ORDER = offsets()


def shifted(me, off, sign):
    z, y, x = me // 16, (me // 4) % 4, me % 4
    dz, dy, dx = [(sign * v) % 4 for v in off]
    return ((z + dz) % 4) * 16 + ((y + dy) % 4) * 4 + (x + dx) % 4


def body(
    q_hbm, k_hbm, v_hbm, sink, wout_hbm, res_hbm, gain_hbm, wg_hbm, wu_hbm, wd_hbm, ids_hbm, rw_hbm,
    out,
    q_v, kv, kmask, vmask, bias, att, attx, wout, res, gain, wg, wu, wd, ids, rw,
    midway, normed, disp, comb, xbuf3, xin3, hid, part, recv, back3, ret3,
    local_sem, halo_s, halo_r, att_s, att_r, d_s, d_r, f_s, f_r, p_s, p_r, r_s, r_r,
):
    me = lax.axis_index("sp")
    t = lax.axis_index("tp")
    other = 1 - t
    xbuf, back, ret = [b.reshape(NSP * PAD, DM) for b in (xbuf3, back3, ret3)]
    xin = xin3.reshape(WAVES * ROWS, DM)
    right = lax.rem(me + 1, NSP)
    left = lax.rem(me + NSP - 1, NSP)

    barrier = pltpu.get_barrier_semaphore()

    @pl.loop(1, NSP)
    def _(i):
        pl.semaphore_signal(
            barrier, inc=1, device_id=(lax.rem(me + i, NSP), t), device_id_type=MESH
        )

    pl.semaphore_signal(barrier, inc=1, device_id=(me, other), device_id_type=MESH)

    loads = [
        (k_hbm, kv.at[0, pl.ds(WIN, 2 * WIN)]),
        (v_hbm, kv.at[1, pl.ds(WIN, 2 * WIN)]),
        (q_hbm, q_v),
        (ids_hbm, ids),
        (rw_hbm, rw),
        (wout_hbm, wout),
        (res_hbm, res),
        (gain_hbm, gain),
        (wg_hbm, wg),
        (wu_hbm, wu),
        (wd_hbm, wd),
    ]
    copies = [
        pltpu.make_async_copy(a, b, local_sem.at[i]) for i, (a, b) in enumerate(loads)
    ]
    for c in copies:
        c.start()

    ret[...] = jnp.zeros_like(ret)

    copies[3].wait()
    copies[4].wait()
    sub = lax.broadcasted_iota(jnp.int32, (NSP, WIN), 0)
    ohs = [(sub == ids[k : k + 1, :]).astype(F32) for k in range(2)]
    before = (
        lax.broadcasted_iota(jnp.int32, (WIN, WIN), 0)
        < lax.broadcasted_iota(jnp.int32, (WIN, WIN), 1)
    ).astype(BF)
    total0 = jnp.sum(ohs[0], axis=1, keepdims=True)
    slot_rows = []
    for k in range(2):
        earlier = jnp.dot(ohs[k].astype(BF), before, preferred_element_type=F32)
        if k == 1:
            earlier = earlier + total0
        rank = jnp.sum(ohs[k] * earlier, axis=0, keepdims=True)
        slot_rows.append(ids[k : k + 1, :] * PAD + rank.astype(jnp.int32))
    srow = lax.broadcasted_iota(jnp.int32, (NSP * PAD, WIN), 0)
    hits = [srow == slot_rows[k] for k in range(2)]
    disp[...] = (hits[0] | hits[1]).astype(F32).astype(BF)
    weight = jnp.where(hits[0], rw[0:1, :], 0.0) + jnp.where(hits[1], rw[1:2, :], 0.0)
    weight = weight.T
    high = weight.astype(BF)
    comb[0] = high
    comb[1] = (weight - high.astype(F32)).astype(BF)

    copies[0].wait()
    copies[1].wait()
    pl.semaphore_wait(barrier, NSP)
    to_left = pltpu.make_async_remote_copy(
        kv.at[:, pl.ds(WIN, WIN)], kv.at[:, pl.ds(3 * WIN, WIN)], halo_s.at[0], halo_r.at[0],
        device_id=(left, t), device_id_type=MESH,
    )
    to_right = pltpu.make_async_remote_copy(
        kv.at[:, pl.ds(2 * WIN, WIN)], kv.at[:, pl.ds(0, WIN)], halo_s.at[1], halo_r.at[1],
        device_id=(right, t), device_id_type=MESH,
    )
    to_left.start()
    to_right.start()

    row = lax.broadcasted_iota(jnp.int32, (WIN, WIN), 0)
    col = lax.broadcasted_iota(jnp.int32, (WIN, WIN), 1)
    bias[0] = jnp.where(col >= row, 0.0, NEG_BIG)
    bias[1] = jnp.where(col <= row, 0.0, NEG_BIG)
    copies[2].wait()
    to_left.wait()
    to_right.wait()

    low = lax.broadcasted_iota(jnp.int32, (4 * WIN, WIN), 1) < 64
    keys = kv[0].astype(F32)
    keys_r = pltpu.roll(keys, 64, 1)
    vals = kv[1].astype(F32)
    vals_r = pltpu.roll(vals, 64, 1)
    ones = jnp.ones_like(keys)
    for g in range(2):
        k_lo, k_hi = (keys, keys_r) if g == 0 else (keys_r, keys)
        v_lo, v_hi = (vals, vals_r) if g == 0 else (vals_r, vals)
        kmask[g, 0] = jnp.where(low, k_lo, 0.0).astype(BF)
        kmask[g, 1] = jnp.where(low, 0.0, k_hi).astype(BF)
        vmask[g, 0, :, 0:WIN] = jnp.where(low, v_lo, 0.0).astype(BF)
        vmask[g, 1, :, 0:WIN] = jnp.where(low, 0.0, v_hi).astype(BF)
        vmask[g, 0, :, WIN:] = jnp.where(low, ones, 0.0).astype(BF)
        vmask[g, 1, :, WIN:] = jnp.where(low, 0.0, ones).astype(BF)

    lane_low = lax.broadcasted_iota(jnp.int32, (WIN, WIN), 1) < 64

    def tile(step, _):
        qt = lax.rem(other + step, 2)
        base = pl.multiple_of(qt * WIN, WIN)
        no_left = jnp.where((me == 0) & (qt == 0), NEG_BIG, 0.0).astype(F32)
        no_right = jnp.where((me == NSP - 1) & (qt == 1), NEG_BIG, 0.0).astype(F32)
        bias_l = bias[0] + no_left
        bias_r = bias[1] + no_right
        for pair in range(4):
            g = pair // 2
            qp = q_v[pl.ds(base, WIN), pair * WIN : (pair + 1) * WIN]
            acc = None
            tail = []
            for side in range(2):
                s = lax.dot_general(
                    qp, kmask[g, side, pl.ds(base, 3 * WIN), :], (((1,), (1,)), ((), ())),
                    preferred_element_type=F32,
                )
                s_l = s[:, 0:WIN] + bias_l
                s_m = s[:, WIN : 2 * WIN]
                s_r = s[:, 2 * WIN :] + bias_r
                logit = sink[2 * pair + side] * 8.0
                peak = jnp.max(
                    jnp.maximum(jnp.maximum(s_l, s_m), s_r), axis=1, keepdims=True
                )
                peak = jnp.maximum(peak, logit)
                expo = jnp.concatenate(
                    [jnp.exp2((v - peak) * EXP_SCALE).astype(BF) for v in (s_l, s_m, s_r)],
                    axis=1,
                )
                o = jnp.dot(
                    expo, vmask[g, side, pl.ds(base, 3 * WIN), :], preferred_element_type=F32
                )
                acc = o if acc is None else acc + o
                tail.append(jnp.exp2((logit - peak) * EXP_SCALE))
            div = acc[:, WIN:] + jnp.where(lane_low, tail[0], tail[1])
            att[pl.ds(base, WIN), pair * WIN : (pair + 1) * WIN] = (
                acc[:, 0:WIN] / div
            ).astype(BF)

        @pl.when(step == 0)
        def _():
            send_att().start()

        return 0

    def send_att():
        return pltpu.make_async_remote_copy(
            att.at[pl.ds(pl.multiple_of(other * WIN, WIN), WIN)], attx, att_s, att_r,
            device_id=(me, other), device_id_type=MESH,
        )

    lax.fori_loop(0, 2, tile, 0)

    copies[5].wait()
    copies[6].wait()
    copies[7].wait()
    send_att().wait()

    mine = pl.multiple_of(t * WIN, WIN)
    w_mine = pl.multiple_of(t * 512, 512)
    w_other = pl.multiple_of(other * 512, 512)
    square = jnp.zeros((WIN, WIN), F32)
    for c in range(8):
        cols = slice(c * 256, (c + 1) * 256)
        proj = jnp.dot(
            att[pl.ds(mine, WIN), :], wout[pl.ds(w_mine, 512), cols], preferred_element_type=F32
        ) + jnp.dot(attx[...], wout[pl.ds(w_other, 512), cols], preferred_element_type=F32)
        mid = res[:, cols].astype(F32) + proj.astype(BF).astype(F32)
        midway[:, cols] = mid
        sq = mid * mid
        square = square + sq[:, 0:WIN] + sq[:, WIN:]
    inv = lax.rsqrt(jnp.sum(square, axis=1, keepdims=True) * (1.0 / DM) + EPSILON)
    for c in range(8):
        cols = slice(c * 256, (c + 1) * 256)
        normed[:, cols] = (midway[:, cols] * inv * gain[:, cols]).astype(BF)
    for c in range(8):
        cols = slice(c * 256, (c + 1) * 256)
        xbuf[:, cols] = jnp.dot(
            disp[...], normed[:, cols], preferred_element_type=F32
        ).astype(BF)

    def wave_rows(w, side):
        return (w * 2 + side) * HALF

    def dispatch(i):
        d = shifted(me, ORDER[i], 1)
        spot = (i // PER * 2 + t) * PER + i % PER
        return pltpu.make_async_remote_copy(
            xbuf3.at[d, pl.ds(0, SLOT)], xin3.at[spot, pl.ds(0, SLOT)],
            d_s.at[i], d_r.at[i], device_id=(d, t), device_id_type=MESH,
        )

    for i in range(1, NSP):
        dispatch(i).start()
    xin[pl.ds(pl.multiple_of(t * HALF, HALF), PAD), :] = xbuf[
        pl.ds(pl.multiple_of(me * PAD, PAD), PAD), :
    ]

    def forward(w):
        rows = pl.ds((w * 2 + t) * PER, PER)
        return pltpu.make_async_remote_copy(
            xin3.at[rows], xin3.at[rows], f_s.at[w], f_r.at[w],
            device_id=(me, other), device_id_type=MESH,
        )

    def halves(w):
        rows = pl.ds(pl.multiple_of(wave_rows(w, other), HALF), HALF)
        return pltpu.make_async_remote_copy(
            part.at[rows], recv.at[pl.ds(w * HALF, HALF)], p_s.at[w], p_r.at[w],
            device_id=(me, other), device_id_type=MESH,
        )

    def give_back(i):
        d = shifted(me, ORDER[i], -1)
        return pltpu.make_async_remote_copy(
            back3.at[i, pl.ds(0, SLOT)], ret3.at[me, pl.ds(0, SLOT)],
            r_s.at[i], r_r.at[i], device_id=(d, t), device_id_type=MESH,
        )

    def arrive(w):
        for i in range(max(1, w * PER), (w + 1) * PER):
            dispatch(i).wait_recv()
        forward(w).start()

    def compute(w):
        forward(w).wait_recv()
        if w == 0:
            copies[8].wait()
            copies[9].wait()
            copies[10].wait()
        rows = slice(w * ROWS, (w + 1) * ROWS)
        for c in range(HID // 256):
            cols = slice(c * 256, (c + 1) * 256)
            gate = jnp.dot(xin[rows, :], wg[:, cols], preferred_element_type=F32)
            up = jnp.dot(xin[rows, :], wu[:, cols], preferred_element_type=F32)
            act = jnp.minimum(gate, CLAMP_LIMIT)
            lin = jnp.clip(up, -CLAMP_LIMIT, CLAMP_LIMIT) + 1.0
            hid[:, cols] = (lin * act * jax.nn.sigmoid(GATE_ALPHA * act)).astype(BF)
        for c in range(DM // 256):
            cols = slice(c * 256, (c + 1) * 256)
            part[rows, cols] = jnp.dot(
                hid[...], wd[:, cols], preferred_element_type=F32
            ).astype(BF)
        halves(w).start()

    def finish(w):
        halves(w).wait_recv()
        own = pl.ds(pl.multiple_of(wave_rows(w, t), HALF), HALF)
        rows = slice(w * HALF, (w + 1) * HALF)
        for c in range(DM // 512):
            cols = slice(c * 512, (c + 1) * 512)
            back[rows, cols] = (
                part[own, cols].astype(F32) + recv[rows, cols].astype(F32)
            ).astype(BF)
        for i in range(max(1, w * PER), (w + 1) * PER):
            give_back(i).start()
        if w == 0:
            ret[pl.ds(pl.multiple_of(me * PAD, PAD), PAD), :] = back[0:PAD, :]

    arrive(0)
    for w in range(WAVES):
        compute(w)
        if w + 1 < WAVES:
            arrive(w + 1)
        finish(w)

    for i in range(1, NSP):
        give_back(i).wait_recv()
    for c in range(8):
        cols = slice(c * 256, (c + 1) * 256)
        routed = jnp.dot(comb[0], ret[:, cols], preferred_element_type=F32) + jnp.dot(
            comb[1], ret[:, cols], preferred_element_type=F32
        )
        out[:, cols] = (midway[:, cols] + routed).astype(BF)

    for i in range(1, NSP):
        dispatch(i).wait_send()
        give_back(i).wait_send()
    for w in range(WAVES):
        forward(w).wait_send()
        halves(w).wait_send()


def per_device(
    queries, keys, values, sink_logit, w_out, residual, norm_gain, w_gate, w_up, w_down,
    expert_ids, route_weight,
):
    any_spec = pl.BlockSpec(memory_space=pl.ANY)
    specs = [any_spec] * 12
    specs[3] = pl.BlockSpec(memory_space=pltpu.SMEM)
    dma = pltpu.SemaphoreType.DMA
    return pl.pallas_call(
        body,
        out_shape=jax.ShapeDtypeStruct((WIN, DM), BF),
        in_specs=specs,
        out_specs=pl.BlockSpec(memory_space=pltpu.VMEM),
        scratch_shapes=[
            pltpu.VMEM((2 * WIN, 512), BF),
            pltpu.VMEM((2, 4 * WIN, WIN), BF),
            pltpu.VMEM((2, 2, 4 * WIN, WIN), BF),
            pltpu.VMEM((2, 2, 4 * WIN, 2 * WIN), BF),
            pltpu.VMEM((2, WIN, WIN), F32),
            pltpu.VMEM((2 * WIN, 512), BF),
            pltpu.VMEM((WIN, 512), BF),
            pltpu.VMEM((1024, DM), BF),
            pltpu.VMEM((WIN, DM), BF),
            pltpu.VMEM((1, DM), F32),
            pltpu.VMEM((DM, HID), BF),
            pltpu.VMEM((DM, HID), BF),
            pltpu.VMEM((HID, DM), BF),
            pltpu.VMEM((2, WIN), jnp.int32),
            pltpu.VMEM((2, WIN), F32),
            pltpu.VMEM((WIN, DM), F32),
            pltpu.VMEM((WIN, DM), BF),
            pltpu.VMEM((NSP * PAD, WIN), BF),
            pltpu.VMEM((2, WIN, NSP * PAD), BF),
            pltpu.VMEM((NSP, PAD, DM), BF),
            pltpu.VMEM((2 * NSP, PAD, DM), BF),
            pltpu.VMEM((ROWS, HID), BF),
            pltpu.VMEM((WAVES * ROWS, DM), BF),
            pltpu.VMEM((NSP * PAD, DM), BF),
            pltpu.VMEM((NSP, PAD, DM), BF),
            pltpu.VMEM((NSP, PAD, DM), BF),
            dma((11,)),
            dma((2,)),
            dma((2,)),
            dma,
            dma,
            dma((NSP,)),
            dma((NSP,)),
            dma((WAVES,)),
            dma((WAVES,)),
            dma((WAVES,)),
            dma((WAVES,)),
            dma((NSP,)),
            dma((NSP,)),
        ],
        compiler_params=pltpu.CompilerParams(
            collective_id=0, has_side_effects=True, vmem_limit_bytes=62 * 2**20
        ),
    )(
        queries, keys, values, sink_logit, w_out, residual, norm_gain.reshape(1, DM),
        w_gate[0], w_up[0], w_down[0], expert_ids.T, route_weight.T,
    )


def solution(mesh):
    in_specs = (
        P("sp", "tp"),
        P("sp", "tp"),
        P("sp", "tp"),
        P("tp"),
        P(),
        P(("sp", "tp"), None),
        P(),
        P("sp", None, "tp"),
        P("sp", None, "tp"),
        P("sp", "tp", None),
        P(("sp", "tp"), None),
        P(("sp", "tp"), None),
    )
    return jax.shard_map(
        per_device,
        mesh=mesh,
        in_specs=in_specs,
        out_specs=P(("sp", "tp"), None),
        check_vma=False,
    )
```

```python
import functools
import random

import jax
import jax.numpy as jnp
import numpy as np
from jax import lax
from jax.experimental import pallas as pl
from jax.experimental.pallas import tpu as pltpu
from jax.sharding import PartitionSpec as P

MESH = pl.DeviceIdType.MESH
BF = jnp.bfloat16
F32 = jnp.float32

NSP = 64
WIN = 128
DM = 2048
HID = 1024
SLOT = 6
TILE = 8
SIZES = (8, 8, 16, 16, 16)
WAVES = len(SIZES)
PLAN = (
    "a0", "u0", "a1", "d0", "u1", "f0", "a2", "d1", "a3", "u2",
    "f1", "a4", "d2", "u3", "f2", "d3", "u4", "f3", "d4", "f4",
)
FIRST = [sum(SIZES[:w]) for w in range(WAVES)]
MOST = max(SIZES)
SLOTS = NSP * SLOT


def pieces(i):
    at, end = i * SLOT, (i + 1) * SLOT
    while at < end:
        upto = min(end, (at // TILE + 1) * TILE)
        yield at // TILE, at % TILE, upto - at
        at = upto
CLAMP_LIMIT = 7.0
GATE_ALPHA = 1.702
EPSILON = 1e-06
NEG_BIG = -1e30
EXP_SCALE = 1.4426950408889634 / 8.0


def offsets():
    every = [(a, b, c) for a in range(4) for b in range(4) for c in range(4)]
    seen, groups = {(0, 0, 0)}, []
    for o in every:
        if o in seen:
            continue
        group = []
        for p in ((0, 1, 2), (1, 2, 0), (2, 0, 1)):
            for s in (1, -1):
                m = tuple((s * o[i]) % 4 for i in p)
                if m not in group:
                    group.append(m)
        seen |= set(group)
        groups.append(group)
    random.Random(1).shuffle(groups)
    groups.sort(key=lambda g: -sum(min(v, 4 - v) for v in g[0]))
    return [(0, 0, 0)] + [o for g in groups for o in g]


ORDER = offsets()


def shifted(me, off, sign):
    z, y, x = me // 16, (me // 4) % 4, me % 4
    dz, dy, dx = [(sign * v) % 4 for v in off]
    return ((z + dz) % 4) * 16 + ((y + dy) % 4) * 4 + (x + dx) % 4


def body(
    q_hbm, k_hbm, v_hbm, sink_hbm, wout_hbm, res_hbm, gain_hbm, wg_hbm, wu_hbm, wd_hbm, ids_hbm, rw_hbm,
    tab_hbm, out,
    q_v, kv, kmask, vmask, bias, near, peaks, att, attx, sink, wout, res, gain, wg, wu, wd, ids, rw, tab,
    midway, normed, disp, comb, xbuf3, xin3, hid, part, recv, back3, ret3,
    local_sem, halo_s, halo_r, att_s, att_r, d_s, d_r, f_s, f_r, p_s, p_r, r_s, r_r,
):
    me = lax.axis_index("sp")
    t = lax.axis_index("tp")
    other = 1 - t
    xbuf, back, ret = [b.reshape(SLOTS, DM) for b in (xbuf3, back3, ret3)]
    xin = xin3.reshape(2 * SLOTS, DM)
    right = lax.rem(me + 1, NSP)
    left = lax.rem(me + NSP - 1, NSP)

    loads = [
        (k_hbm, kv.at[0, pl.ds(WIN, 2 * WIN)]),
        (v_hbm, kv.at[1, pl.ds(WIN, 2 * WIN)]),
        (q_hbm, q_v),
        (ids_hbm, ids),
        (rw_hbm, rw),
        (wout_hbm, wout),
        (res_hbm, res),
        (gain_hbm, gain),
        (wg_hbm, wg),
        (wu_hbm, wu),
        (wd_hbm, wd),
        (tab_hbm, tab),
        (sink_hbm, sink),
    ]
    copies = [
        pltpu.make_async_copy(a, b, local_sem.at[i]) for i, (a, b) in enumerate(loads)
    ]
    for i in (0, 1, 2, 12, 3, 4, 11, 6, 7, 5, 8, 9, 10):
        copies[i].start()

    barrier = pltpu.get_barrier_semaphore()
    pl.semaphore_signal(barrier, inc=1, device_id=(left, t), device_id_type=MESH)
    pl.semaphore_signal(barrier, inc=1, device_id=(right, t), device_id_type=MESH)
    pl.semaphore_signal(barrier, inc=1, device_id=(me, other), device_id_type=MESH)
    for i in range(2, NSP - 1):
        pl.semaphore_signal(
            barrier, inc=1, device_id=(lax.rem(me + i, NSP), t), device_id_type=MESH
        )

    row = lax.broadcasted_iota(jnp.int32, (WIN, WIN), 0)
    col = lax.broadcasted_iota(jnp.int32, (WIN, WIN), 1)
    for i in (3, 4, 11):
        copies[i].wait()
    ret[...] = jnp.zeros_like(ret)
    sub = lax.broadcasted_iota(jnp.int32, (NSP, WIN), 0)
    ohs = [(sub == ids[k : k + 1, :]).astype(F32) for k in range(2)]
    before = (row < col).astype(F32).astype(BF)
    total0 = jnp.sum(ohs[0], axis=1, keepdims=True)
    slot_rows = []
    for k in range(2):
        earlier = jnp.dot(ohs[k].astype(BF), before, preferred_element_type=F32)
        if k == 1:
            earlier = earlier + total0
        rank = jnp.sum(ohs[k] * earlier, axis=0, keepdims=True)
        slot_rows.append(ids[k : k + 1, :] * SLOT + rank.astype(jnp.int32))
    offs = tab[...] >> 3
    there = (
        ((me // 16 + offs // 16) & 3) * 16
        + (((me // 4) % 4 + offs // 4) & 3) * 4
        + ((me % 4 + offs) & 3)
    )
    srow = there * SLOT + (tab[...] & 7)
    hits = [srow == slot_rows[k] for k in range(2)]
    disp[...] = (hits[0] | hits[1]).astype(F32).astype(BF)

    copies[0].wait()
    copies[1].wait()
    pl.semaphore_wait(barrier, NSP)
    to_left = pltpu.make_async_remote_copy(
        kv.at[:, pl.ds(WIN, WIN)], kv.at[:, pl.ds(3 * WIN, WIN)], halo_s.at[0], halo_r.at[0],
        device_id=(left, t), device_id_type=MESH,
    )
    to_right = pltpu.make_async_remote_copy(
        kv.at[:, pl.ds(2 * WIN, WIN)], kv.at[:, pl.ds(0, WIN)], halo_s.at[1], halo_r.at[1],
        device_id=(right, t), device_id_type=MESH,
    )
    to_left.start()
    to_right.start()

    bias[0] = jnp.where(col >= row, 0.0, NEG_BIG)
    bias[1] = jnp.where(col <= row, 0.0, NEG_BIG)

    def spread(lo, size):
        rows = slice(lo, lo + size)
        low = lax.broadcasted_iota(jnp.int32, (size, WIN), 1) < 64
        keys = kv[0, rows].astype(F32)
        keys_r = pltpu.roll(keys, 64, 1)
        vals = kv[1, rows].astype(F32)
        vals_r = pltpu.roll(vals, 64, 1)
        ones = jnp.ones_like(keys)
        for g in range(2):
            k_lo, k_hi = (keys, keys_r) if g == 0 else (keys_r, keys)
            v_lo, v_hi = (vals, vals_r) if g == 0 else (vals_r, vals)
            kmask[g, 0, rows] = jnp.where(low, k_lo, 0.0).astype(BF)
            kmask[g, 1, rows] = jnp.where(low, 0.0, k_hi).astype(BF)
            vmask[g, 0, rows, 0:WIN] = jnp.where(low, v_lo, 0.0).astype(BF)
            vmask[g, 1, rows, 0:WIN] = jnp.where(low, 0.0, v_hi).astype(BF)
            vmask[g, 0, rows, WIN:] = jnp.where(low, ones, 0.0).astype(BF)
            vmask[g, 1, rows, WIN:] = jnp.where(low, 0.0, ones).astype(BF)

    spread(WIN, 2 * WIN)
    copies[2].wait()
    copies[12].wait()

    lane_low = lax.broadcasted_iota(jnp.int32, (WIN, WIN), 1) < 64

    def scores(qp, keys):
        return lax.dot_general(
            qp, keys, (((1,), (1,)), ((), ())), preferred_element_type=F32
        )

    def own_tile(qt, _):
        base = pl.multiple_of(qt * WIN, WIN)
        cut_a = jnp.where(qt == 1, bias[0], 0.0)
        cut_b = jnp.where(qt == 0, bias[1], 0.0)
        for pair in range(4):
            g = pair // 2
            qp = q_v[pl.ds(base, WIN), pair * WIN : (pair + 1) * WIN]
            acc = None
            for side in range(2):
                s = scores(qp, kmask[g, side, WIN : 3 * WIN, :])
                s_a = s[:, 0:WIN] + cut_a
                s_b = s[:, WIN:] + cut_b
                logit = sink[2 * pair + side] * 8.0
                peak = jnp.max(jnp.maximum(s_a, s_b), axis=1, keepdims=True)
                peak = jnp.maximum(peak, logit)
                expo = jnp.concatenate(
                    [jnp.exp2((v - peak) * EXP_SCALE).astype(BF) for v in (s_a, s_b)], axis=1
                )
                o = jnp.dot(
                    expo, vmask[g, side, WIN : 3 * WIN, :], preferred_element_type=F32
                )
                acc = o if acc is None else acc + o
                peaks[qt, pair, side] = jnp.broadcast_to(peak, (WIN, WIN))
            near[qt, pair] = acc
        return 0

    lax.fori_loop(0, 2, own_tile, 0)

    to_left.wait()
    to_right.wait()
    spread(0, WIN)
    spread(3 * WIN, WIN)

    def far_tile(step, _):
        qt = lax.rem(other + step, 2)
        base = pl.multiple_of(qt * WIN, WIN)
        edge = ((me == 0) & (qt == 0)) | ((me == NSP - 1) & (qt == 1))
        cut = jnp.where(qt == 0, bias[0], bias[1]) + jnp.where(edge, NEG_BIG, 0.0)
        keys_at = pl.ds(pl.multiple_of(qt * 3 * WIN, WIN), WIN)
        for pair in range(4):
            g = pair // 2
            qp = q_v[pl.ds(base, WIN), pair * WIN : (pair + 1) * WIN]
            acc = None
            peaks_now = []
            for side in range(2):
                s = scores(qp, kmask[g, side, keys_at, :]) + cut
                peak = jnp.maximum(
                    peaks[qt, pair, side], jnp.max(s, axis=1, keepdims=True)
                )
                expo = jnp.exp2((s - peak) * EXP_SCALE).astype(BF)
                o = jnp.dot(expo, vmask[g, side, keys_at, :], preferred_element_type=F32)
                acc = o if acc is None else acc + o
                peaks_now.append(peak)
            top = jnp.where(lane_low, peaks[qt, pair, 0], peaks[qt, pair, 1])
            peak = jnp.where(lane_low, peaks_now[0], peaks_now[1])
            logit = jnp.where(lane_low, sink[2 * pair], sink[2 * pair + 1]) * 8.0
            fade = jnp.exp2((top - peak) * EXP_SCALE)
            tail = jnp.exp2((logit - peak) * EXP_SCALE)
            div = near[qt, pair, :, WIN:] * fade + acc[:, WIN:] + tail
            att[pl.ds(base, WIN), pair * WIN : (pair + 1) * WIN] = (
                (near[qt, pair, :, 0:WIN] * fade + acc[:, 0:WIN]) / div
            ).astype(BF)

        @pl.when(step == 0)
        def _():
            send_att().start()

        return 0

    def send_att():
        return pltpu.make_async_remote_copy(
            att.at[pl.ds(pl.multiple_of(other * WIN, WIN), WIN)], attx, att_s, att_r,
            device_id=(me, other), device_id_type=MESH,
        )

    lax.fori_loop(0, 2, far_tile, 0)

    for i in (5, 6, 7):
        copies[i].wait()
    mine = pl.multiple_of(t * WIN, WIN)
    w_mine = pl.multiple_of(t * 512, 512)
    w_other = pl.multiple_of(other * 512, 512)
    for c in range(8):
        cols = slice(c * 256, (c + 1) * 256)
        midway[:, cols] = jnp.dot(
            att[pl.ds(mine, WIN), :], wout[pl.ds(w_mine, 512), cols], preferred_element_type=F32
        )
    send_att().wait()

    square = jnp.zeros((WIN, WIN), F32)
    for c in range(8):
        cols = slice(c * 256, (c + 1) * 256)
        proj = midway[:, cols] + jnp.dot(
            attx[...], wout[pl.ds(w_other, 512), cols], preferred_element_type=F32
        )
        mid = res[:, cols].astype(F32) + proj.astype(BF).astype(F32)
        midway[:, cols] = mid
        sq = mid * mid
        square = square + sq[:, 0:WIN] + sq[:, WIN:]
    inv = lax.rsqrt(jnp.sum(square, axis=1, keepdims=True) * (1.0 / DM) + EPSILON)
    for c in range(8):
        cols = slice(c * 256, (c + 1) * 256)
        normed[:, cols] = (midway[:, cols] * inv * gain[:, cols]).astype(BF)

    def tiles(count):
        return count * SLOT // TILE

    def dispatch(i):
        d = shifted(me, ORDER[i], 1)
        w = max(v for v in range(WAVES) if FIRST[v] <= i)
        shift = tiles(FIRST[w]) + t * tiles(SIZES[w])
        return [
            pltpu.make_async_remote_copy(
                xbuf3.at[tile, pl.ds(row, rows)], xin3.at[tile + shift, pl.ds(row, rows)],
                d_s, d_r.at[w], device_id=(d, t), device_id_type=MESH,
            )
            for tile, row, rows in pieces(i)
        ]

    def bulk(ref, count, send_sem, recv_sem):
        rows = ref.at[pl.ds(0, count), pl.ds(0, SLOT)]
        return pltpu.make_async_remote_copy(
            rows, rows, send_sem, recv_sem, device_id=(me, other), device_id_type=MESH
        )

    for w in range(WAVES):
        rows = slice(FIRST[w] * SLOT, (FIRST[w] + SIZES[w]) * SLOT)
        for c in range(8):
            cols = slice(c * 256, (c + 1) * 256)
            xbuf[rows, cols] = jnp.dot(
                disp[rows, :], normed[:, cols], preferred_element_type=F32
            ).astype(BF)
        for i in range(max(1, FIRST[w]), FIRST[w] + SIZES[w]):
            for copy in dispatch(i):
                copy.start()
    xin[pl.ds(pl.multiple_of(t * SIZES[0] * SLOT, TILE), SLOT), :] = xbuf[0:SLOT, :]
    weight = jnp.where(hits[0], rw[0:1, :], 0.0) + jnp.where(hits[1], rw[1:2, :], 0.0)
    for part_of in range(2):
        turned = weight[part_of * SLOTS // 2 : (part_of + 1) * SLOTS // 2].T
        high = turned.astype(BF)
        comb[part_of, 0] = high
        comb[part_of, 1] = (turned - high.astype(F32)).astype(BF)

    def wave_rows(w, side):
        return pl.multiple_of((2 * FIRST[w] + side * SIZES[w]) * SLOT, 8 * SLOT)

    def forward(w):
        rows = pl.ds(2 * tiles(FIRST[w]) + t * tiles(SIZES[w]), tiles(SIZES[w]))
        return pltpu.make_async_remote_copy(
            xin3.at[rows], xin3.at[rows], f_s.at[w], f_r.at[w],
            device_id=(me, other), device_id_type=MESH,
        )

    def halves(w):
        rows = pl.ds(wave_rows(w, other), SIZES[w] * SLOT)
        return pltpu.make_async_remote_copy(
            part.at[rows], recv.at[pl.ds(FIRST[w] * SLOT, SIZES[w] * SLOT)], p_s.at[w], p_r.at[w],
            device_id=(me, other), device_id_type=MESH,
        )

    def give_back(i):
        d = shifted(me, ORDER[i], -1)
        return [
            pltpu.make_async_remote_copy(
                back3.at[tile, pl.ds(row, rows)], ret3.at[tile, pl.ds(row, rows)],
                r_s, r_r.at[int(i >= NSP // 2)], device_id=(d, t), device_id_type=MESH,
            )
            for tile, row, rows in pieces(i)
        ]

    def arrive(w):
        bulk(xin3, SIZES[w] - (w == 0), d_s, d_r.at[w]).wait_recv()
        forward(w).start()

    def gate_up(w):
        forward(w).wait_recv()
        if w == 0:
            for i in (8, 9, 10):
                copies[i].wait()
        rows = slice(2 * FIRST[w] * SLOT, 2 * (FIRST[w] + SIZES[w]) * SLOT)
        for c in range(HID // 256):
            cols = slice(c * 256, (c + 1) * 256)
            gate = jnp.dot(xin[rows, :], wg[:, cols], preferred_element_type=F32)
            up = jnp.dot(xin[rows, :], wu[:, cols], preferred_element_type=F32)
            act = jnp.minimum(gate, CLAMP_LIMIT)
            lin = jnp.clip(up, -CLAMP_LIMIT, CLAMP_LIMIT) + 1.0
            hid[0 : 2 * SIZES[w] * SLOT, cols] = (lin * act * jax.nn.sigmoid(GATE_ALPHA * act)).astype(BF)

    def down(w):
        rows = slice(2 * FIRST[w] * SLOT, 2 * (FIRST[w] + SIZES[w]) * SLOT)
        for c in range(DM // 256):
            cols = slice(c * 256, (c + 1) * 256)
            part[rows, cols] = jnp.dot(
                hid[0 : 2 * SIZES[w] * SLOT, :], wd[:, cols], preferred_element_type=F32
            ).astype(BF)
        halves(w).start()

    def finish(w):
        halves(w).wait_recv()
        own = pl.ds(wave_rows(w, t), SIZES[w] * SLOT)
        rows = slice(FIRST[w] * SLOT, (FIRST[w] + SIZES[w]) * SLOT)
        for c in range(DM // 512):
            cols = slice(c * 512, (c + 1) * 512)
            back[rows, cols] = (
                part[own, cols].astype(F32) + recv[rows, cols].astype(F32)
            ).astype(BF)
        for i in range(max(1, FIRST[w]), FIRST[w] + SIZES[w]):
            for copy in give_back(i):
                copy.start()
        if w == 0:
            ret[0:SLOT, :] = back[0:SLOT, :]

    steps = {"a": arrive, "u": gate_up, "d": down, "f": finish}
    for step in PLAN:
        steps[step[0]](int(step[1:]))

    def combine(part_of):
        rows = slice(part_of * SLOTS // 2, (part_of + 1) * SLOTS // 2)
        for c in range(8):
            cols = slice(c * 256, (c + 1) * 256)
            total = midway[:, cols]
            for k in range(2):
                total = total + jnp.dot(
                    comb[part_of, k], ret[rows, cols], preferred_element_type=F32
                )
            if part_of == 1:
                out[:, cols] = total.astype(BF)
            else:
                midway[:, cols] = total

    bulk(xin3, NSP - 1, d_s, d_r.at[0]).wait_send()
    for w in range(WAVES):
        forward(w).wait_send()
        halves(w).wait_send()
    bulk(xin3, NSP // 2 - 1, r_s, r_r.at[0]).wait_recv()
    combine(0)
    bulk(xin3, NSP // 2, r_s, r_r.at[1]).wait_recv()
    combine(1)
    bulk(xin3, NSP - 1, r_s, r_r.at[0]).wait_send()


def per_device(
    queries, keys, values, sink_logit, w_out, residual, norm_gain, w_gate, w_up, w_down,
    expert_ids, route_weight,
):
    any_spec = pl.BlockSpec(memory_space=pltpu.HBM)
    specs = [any_spec] * 13
    code = [dz * 16 + dy * 4 + dx for dz, dy, dx in ORDER]
    rows = [c * 8 + j for c in code for j in range(SLOT)]
    table = np.array(rows, np.int32)[:, None].repeat(WIN, 1)
    dma = pltpu.SemaphoreType.DMA
    return pl.pallas_call(
        body,
        out_shape=pltpu.VMEM((WIN, DM), BF),
        in_specs=specs,
        out_specs=pl.BlockSpec(memory_space=pltpu.VMEM),
        scratch_shapes=[
            pltpu.VMEM((2 * WIN, 512), BF),
            pltpu.VMEM((2, 4 * WIN, WIN), BF),
            pltpu.VMEM((2, 2, 4 * WIN, WIN), BF),
            pltpu.VMEM((2, 2, 4 * WIN, 2 * WIN), BF),
            pltpu.VMEM((2, WIN, WIN), F32),
            pltpu.VMEM((2, 4, WIN, 2 * WIN), F32),
            pltpu.VMEM((2, 4, 2, WIN, WIN), F32),
            pltpu.VMEM((2 * WIN, 512), BF),
            pltpu.VMEM((WIN, 512), BF),
            pltpu.SMEM((8,), F32),
            pltpu.VMEM((1024, DM), BF),
            pltpu.VMEM((WIN, DM), BF),
            pltpu.VMEM((1, DM), F32),
            pltpu.VMEM((DM, HID), BF),
            pltpu.VMEM((DM, HID), BF),
            pltpu.VMEM((HID, DM), BF),
            pltpu.VMEM((2, WIN), jnp.int32),
            pltpu.VMEM((2, WIN), F32),
            pltpu.VMEM((SLOTS, WIN), jnp.int32),
            pltpu.VMEM((WIN, DM), F32),
            pltpu.VMEM((WIN, DM), BF),
            pltpu.VMEM((SLOTS, WIN), BF),
            pltpu.VMEM((2, 2, WIN, SLOTS // 2), BF),
            pltpu.VMEM((SLOTS // TILE, TILE, DM), BF),
            pltpu.VMEM((2 * SLOTS // TILE, TILE, DM), BF),
            pltpu.VMEM((2 * MOST * SLOT, HID), BF),
            pltpu.VMEM((2 * SLOTS, DM), BF),
            pltpu.VMEM((SLOTS, DM), BF),
            pltpu.VMEM((SLOTS // TILE, TILE, DM), BF),
            pltpu.VMEM((SLOTS // TILE, TILE, DM), BF),
            dma((13,)),
            dma((2,)),
            dma((2,)),
            dma,
            dma,
            dma,
            dma((WAVES,)),
            dma((WAVES,)),
            dma((WAVES,)),
            dma((WAVES,)),
            dma((WAVES,)),
            dma,
            dma((2,)),
        ],
        compiler_params=pltpu.CompilerParams(
            collective_id=0, has_side_effects=True, vmem_limit_bytes=58 * 2**20
        ),
    )(
        queries, keys, values, sink_logit, w_out, residual, norm_gain.reshape(1, DM),
        w_gate[0], w_up[0], w_down[0], expert_ids.T, route_weight.T, jnp.asarray(table),
    )


def solution(mesh):
    in_specs = (
        P("sp", "tp"),
        P("sp", "tp"),
        P("sp", "tp"),
        P("tp"),
        P(),
        P(("sp", "tp"), None),
        P(),
        P("sp", None, "tp"),
        P("sp", None, "tp"),
        P("sp", "tp", None),
        P(("sp", "tp"), None),
        P(("sp", "tp"), None),
    )
    return jax.shard_map(
        per_device,
        mesh=mesh,
        in_specs=in_specs,
        out_specs=P(("sp", "tp"), None),
        check_vma=False,
    )
```

```python
import functools
import random

import jax
import jax.numpy as jnp
import numpy as np
from jax import lax
from jax.experimental import pallas as pl
from jax.experimental.pallas import tpu as pltpu
from jax.sharding import PartitionSpec as P

MESH = pl.DeviceIdType.MESH
BF = jnp.bfloat16
F32 = jnp.float32

NSP = 64
WIN = 128
DM = 2048
HID = 1024
SLOT = 6
TILE = 8
SIZES = (8, 8, 16, 16, 16)
WAVES = len(SIZES)
PLAN = (
    "a0", "u0", "a1", "d0", "u1", "f0", "a2", "d1", "a3", "u2",
    "f1", "d2", "a4", "u3", "f2", "d3", "u4", "f3", "d4", "f4",
)
FIRST = [sum(SIZES[:w]) for w in range(WAVES)]
MOST = max(SIZES)
SLOTS = NSP * SLOT


def pieces(i):
    at, end = i * SLOT, (i + 1) * SLOT
    while at < end:
        upto = min(end, (at // TILE + 1) * TILE)
        yield at // TILE, at % TILE, upto - at
        at = upto
CLAMP_LIMIT = 7.0
GATE_ALPHA = 1.702
EPSILON = 1e-06
NEG_BIG = -1e30
EXP_SCALE = 1.4426950408889634 / 8.0


def offsets():
    every = [(a, b, c) for a in range(4) for b in range(4) for c in range(4)]
    seen, groups = {(0, 0, 0)}, []
    for o in every:
        if o in seen:
            continue
        group = []
        for p in ((0, 1, 2), (1, 2, 0), (2, 0, 1)):
            for s in (1, -1):
                m = tuple((s * o[i]) % 4 for i in p)
                if m not in group:
                    group.append(m)
        seen |= set(group)
        groups.append(group)
    random.Random(1).shuffle(groups)
    groups.sort(key=lambda g: -sum(min(v, 4 - v) for v in g[0]))
    return [(0, 0, 0)] + [o for g in groups for o in g]


ORDER = offsets()


def shifted(me, off, sign):
    z, y, x = me // 16, (me // 4) % 4, me % 4
    dz, dy, dx = [(sign * v) % 4 for v in off]
    return ((z + dz) % 4) * 16 + ((y + dy) % 4) * 4 + (x + dx) % 4


def body(
    q_hbm, k_hbm, v_hbm, sink_hbm, wout_hbm, res_hbm, gain_hbm, wg_hbm, wu_hbm, wd_hbm, ids_hbm, rw_hbm,
    tab_hbm, out,
    q_v, kv, kmask, vmask, bias, near, peaks, att, attx, sink, wout, res, gain, wg, wu, wd, ids, rw, tab,
    midway, normed, disp, comb, xbuf3, xin3, hid, part, recv, back3, ret3,
    local_sem, halo_s, halo_r, att_s, att_r, d_s, d_r, f_s, f_r, p_s, p_r, r_s, r_r,
):
    me = lax.axis_index("sp")
    t = lax.axis_index("tp")
    other = 1 - t
    xbuf, back, ret = [b.reshape(SLOTS, DM) for b in (xbuf3, back3, ret3)]
    xin = xin3.reshape(2 * SLOTS, DM)
    right = lax.rem(me + 1, NSP)
    left = lax.rem(me + NSP - 1, NSP)

    loads = [
        (k_hbm, kv.at[0, pl.ds(WIN, 2 * WIN)]),
        (v_hbm, kv.at[1, pl.ds(WIN, 2 * WIN)]),
        (q_hbm, q_v),
        (ids_hbm, ids),
        (rw_hbm, rw),
        (wout_hbm, wout),
        (res_hbm, res),
        (gain_hbm, gain),
        (wg_hbm, wg),
        (wu_hbm, wu),
        (wd_hbm, wd),
        (tab_hbm, tab),
        (sink_hbm, sink),
    ]
    copies = [
        pltpu.make_async_copy(a, b, local_sem.at[i]) for i, (a, b) in enumerate(loads)
    ]
    for i in (0, 1, 2, 12, 3, 4, 11, 6, 7, 5, 8, 9, 10):
        copies[i].start()

    barrier = pltpu.get_barrier_semaphore()
    pl.semaphore_signal(barrier, inc=1, device_id=(left, t), device_id_type=MESH)
    pl.semaphore_signal(barrier, inc=1, device_id=(right, t), device_id_type=MESH)
    pl.semaphore_signal(barrier, inc=1, device_id=(me, other), device_id_type=MESH)
    for i in range(2, NSP - 1):
        pl.semaphore_signal(
            barrier, inc=1, device_id=(lax.rem(me + i, NSP), t), device_id_type=MESH
        )

    row = lax.broadcasted_iota(jnp.int32, (WIN, WIN), 0)
    col = lax.broadcasted_iota(jnp.int32, (WIN, WIN), 1)
    for i in (3, 4, 11):
        copies[i].wait()
    ret[...] = jnp.zeros_like(ret)
    sub = lax.broadcasted_iota(jnp.int32, (NSP, WIN), 0)
    ohs = [(sub == ids[k : k + 1, :]).astype(F32) for k in range(2)]
    before = (row < col).astype(F32).astype(BF)
    total0 = jnp.sum(ohs[0], axis=1, keepdims=True)
    slot_rows = []
    for k in range(2):
        earlier = jnp.dot(ohs[k].astype(BF), before, preferred_element_type=F32)
        if k == 1:
            earlier = earlier + total0
        rank = jnp.sum(ohs[k] * earlier, axis=0, keepdims=True)
        slot_rows.append(ids[k : k + 1, :] * SLOT + rank.astype(jnp.int32))
    offs = tab[...] >> 3
    there = (
        ((me // 16 + offs // 16) & 3) * 16
        + (((me // 4) % 4 + offs // 4) & 3) * 4
        + ((me % 4 + offs) & 3)
    )
    srow = there * SLOT + (tab[...] & 7)
    hits = [srow == slot_rows[k] for k in range(2)]
    disp[...] = (hits[0] | hits[1]).astype(F32).astype(BF)

    copies[0].wait()
    copies[1].wait()
    pl.semaphore_wait(barrier, NSP)
    to_left = pltpu.make_async_remote_copy(
        kv.at[:, pl.ds(WIN, WIN)], kv.at[:, pl.ds(3 * WIN, WIN)], halo_s.at[0], halo_r.at[0],
        device_id=(left, t), device_id_type=MESH,
    )
    to_right = pltpu.make_async_remote_copy(
        kv.at[:, pl.ds(2 * WIN, WIN)], kv.at[:, pl.ds(0, WIN)], halo_s.at[1], halo_r.at[1],
        device_id=(right, t), device_id_type=MESH,
    )
    to_left.start()
    to_right.start()

    bias[0] = jnp.where(col >= row, 0.0, NEG_BIG)
    bias[1] = jnp.where(col <= row, 0.0, NEG_BIG)

    def spread(lo, size):
        rows = slice(lo, lo + size)
        low = lax.broadcasted_iota(jnp.int32, (size, WIN), 1) < 64
        keys = kv[0, rows].astype(F32)
        keys_r = pltpu.roll(keys, 64, 1)
        vals = kv[1, rows].astype(F32)
        vals_r = pltpu.roll(vals, 64, 1)
        ones = jnp.ones_like(keys)
        for g in range(2):
            k_lo, k_hi = (keys, keys_r) if g == 0 else (keys_r, keys)
            v_lo, v_hi = (vals, vals_r) if g == 0 else (vals_r, vals)
            kmask[g, 0, rows] = jnp.where(low, k_lo, 0.0).astype(BF)
            kmask[g, 1, rows] = jnp.where(low, 0.0, k_hi).astype(BF)
            vmask[g, 0, rows, 0:WIN] = jnp.where(low, v_lo, 0.0).astype(BF)
            vmask[g, 1, rows, 0:WIN] = jnp.where(low, 0.0, v_hi).astype(BF)
            vmask[g, 0, rows, WIN:] = jnp.where(low, ones, 0.0).astype(BF)
            vmask[g, 1, rows, WIN:] = jnp.where(low, 0.0, ones).astype(BF)

    spread(WIN, 2 * WIN)
    copies[2].wait()
    copies[12].wait()

    lane_low = lax.broadcasted_iota(jnp.int32, (WIN, WIN), 1) < 64

    def scores(qp, keys):
        return lax.dot_general(
            qp, keys, (((1,), (1,)), ((), ())), preferred_element_type=F32
        )

    def own_tile(qt, _):
        base = pl.multiple_of(qt * WIN, WIN)
        cut_a = jnp.where(qt == 1, bias[0], 0.0)
        cut_b = jnp.where(qt == 0, bias[1], 0.0)
        for pair in range(4):
            g = pair // 2
            qp = q_v[pl.ds(base, WIN), pair * WIN : (pair + 1) * WIN]
            acc = None
            for side in range(2):
                s = scores(qp, kmask[g, side, WIN : 3 * WIN, :])
                s_a = s[:, 0:WIN] + cut_a
                s_b = s[:, WIN:] + cut_b
                logit = sink[2 * pair + side] * 8.0
                peak = jnp.max(jnp.maximum(s_a, s_b), axis=1, keepdims=True)
                peak = jnp.maximum(peak, logit)
                expo = jnp.concatenate(
                    [jnp.exp2((v - peak) * EXP_SCALE).astype(BF) for v in (s_a, s_b)], axis=1
                )
                o = jnp.dot(
                    expo, vmask[g, side, WIN : 3 * WIN, :], preferred_element_type=F32
                )
                acc = o if acc is None else acc + o
                peaks[qt, pair, side] = jnp.broadcast_to(peak, (WIN, WIN))
            near[qt, pair] = acc
        return 0

    lax.fori_loop(0, 2, own_tile, 0)

    to_left.wait()
    to_right.wait()
    spread(0, WIN)
    spread(3 * WIN, WIN)

    def far_tile(step, _):
        qt = lax.rem(other + step, 2)
        base = pl.multiple_of(qt * WIN, WIN)
        edge = ((me == 0) & (qt == 0)) | ((me == NSP - 1) & (qt == 1))
        cut = jnp.where(qt == 0, bias[0], bias[1]) + jnp.where(edge, NEG_BIG, 0.0)
        keys_at = pl.ds(pl.multiple_of(qt * 3 * WIN, WIN), WIN)
        for pair in range(4):
            g = pair // 2
            qp = q_v[pl.ds(base, WIN), pair * WIN : (pair + 1) * WIN]
            acc = None
            peaks_now = []
            for side in range(2):
                s = scores(qp, kmask[g, side, keys_at, :]) + cut
                peak = jnp.maximum(
                    peaks[qt, pair, side], jnp.max(s, axis=1, keepdims=True)
                )
                expo = jnp.exp2((s - peak) * EXP_SCALE).astype(BF)
                o = jnp.dot(expo, vmask[g, side, keys_at, :], preferred_element_type=F32)
                acc = o if acc is None else acc + o
                peaks_now.append(peak)
            top = jnp.where(lane_low, peaks[qt, pair, 0], peaks[qt, pair, 1])
            peak = jnp.where(lane_low, peaks_now[0], peaks_now[1])
            logit = jnp.where(lane_low, sink[2 * pair], sink[2 * pair + 1]) * 8.0
            fade = jnp.exp2((top - peak) * EXP_SCALE)
            tail = jnp.exp2((logit - peak) * EXP_SCALE)
            div = near[qt, pair, :, WIN:] * fade + acc[:, WIN:] + tail
            att[pl.ds(base, WIN), pair * WIN : (pair + 1) * WIN] = (
                (near[qt, pair, :, 0:WIN] * fade + acc[:, 0:WIN]) / div
            ).astype(BF)

        @pl.when(step == 0)
        def _():
            send_att().start()

        return 0

    def send_att():
        return pltpu.make_async_remote_copy(
            att.at[pl.ds(pl.multiple_of(other * WIN, WIN), WIN)], attx, att_s, att_r,
            device_id=(me, other), device_id_type=MESH,
        )

    lax.fori_loop(0, 2, far_tile, 0)

    for i in (5, 6, 7):
        copies[i].wait()
    mine = pl.multiple_of(t * WIN, WIN)
    w_mine = pl.multiple_of(t * 512, 512)
    w_other = pl.multiple_of(other * 512, 512)
    for c in range(8):
        cols = slice(c * 256, (c + 1) * 256)
        midway[:, cols] = jnp.dot(
            att[pl.ds(mine, WIN), :], wout[pl.ds(w_mine, 512), cols], preferred_element_type=F32
        )
    send_att().wait()

    square = jnp.zeros((WIN, WIN), F32)
    for c in range(8):
        cols = slice(c * 256, (c + 1) * 256)
        proj = midway[:, cols] + jnp.dot(
            attx[...], wout[pl.ds(w_other, 512), cols], preferred_element_type=F32
        )
        mid = res[:, cols].astype(F32) + proj.astype(BF).astype(F32)
        midway[:, cols] = mid
        sq = mid * mid
        square = square + sq[:, 0:WIN] + sq[:, WIN:]
    inv = lax.rsqrt(jnp.sum(square, axis=1, keepdims=True) * (1.0 / DM) + EPSILON)
    for c in range(8):
        cols = slice(c * 256, (c + 1) * 256)
        normed[:, cols] = (midway[:, cols] * inv * gain[:, cols]).astype(BF)

    def tiles(count):
        return count * SLOT // TILE

    def dispatch(i):
        d = shifted(me, ORDER[i], 1)
        w = max(v for v in range(WAVES) if FIRST[v] <= i)
        shift = tiles(FIRST[w]) + t * tiles(SIZES[w])
        return [
            pltpu.make_async_remote_copy(
                xbuf3.at[tile, pl.ds(row, rows)], xin3.at[tile + shift, pl.ds(row, rows)],
                d_s, d_r.at[w], device_id=(d, t), device_id_type=MESH,
            )
            for tile, row, rows in pieces(i)
        ]

    def bulk(ref, count, send_sem, recv_sem):
        rows = ref.at[pl.ds(0, count), pl.ds(0, SLOT)]
        return pltpu.make_async_remote_copy(
            rows, rows, send_sem, recv_sem, device_id=(me, other), device_id_type=MESH
        )

    for w in range(WAVES):
        rows = slice(FIRST[w] * SLOT, (FIRST[w] + SIZES[w]) * SLOT)
        for c in range(8):
            cols = slice(c * 256, (c + 1) * 256)
            xbuf[rows, cols] = jnp.dot(
                disp[rows, :], normed[:, cols], preferred_element_type=F32
            ).astype(BF)
        for i in range(max(1, FIRST[w]), FIRST[w] + SIZES[w]):
            for copy in dispatch(i):
                copy.start()
    xin[pl.ds(pl.multiple_of(t * SIZES[0] * SLOT, TILE), SLOT), :] = xbuf[0:SLOT, :]
    weight = jnp.where(hits[0], rw[0:1, :], 0.0) + jnp.where(hits[1], rw[1:2, :], 0.0)
    for part_of in range(2):
        turned = weight[part_of * SLOTS // 2 : (part_of + 1) * SLOTS // 2].T
        high = turned.astype(BF)
        comb[part_of, 0] = high
        comb[part_of, 1] = (turned - high.astype(F32)).astype(BF)

    def wave_rows(w, side):
        return pl.multiple_of((2 * FIRST[w] + side * SIZES[w]) * SLOT, 8 * SLOT)

    def forward(w):
        rows = pl.ds(2 * tiles(FIRST[w]) + t * tiles(SIZES[w]), tiles(SIZES[w]))
        return pltpu.make_async_remote_copy(
            xin3.at[rows], xin3.at[rows], f_s.at[w], f_r.at[w],
            device_id=(me, other), device_id_type=MESH,
        )

    def halves(w):
        rows = pl.ds(wave_rows(w, other), SIZES[w] * SLOT)
        return pltpu.make_async_remote_copy(
            part.at[rows], recv.at[pl.ds(FIRST[w] * SLOT, SIZES[w] * SLOT)], p_s.at[w], p_r.at[w],
            device_id=(me, other), device_id_type=MESH,
        )

    def give_back(i):
        d = shifted(me, ORDER[i], -1)
        return [
            pltpu.make_async_remote_copy(
                back3.at[tile, pl.ds(row, rows)], ret3.at[tile, pl.ds(row, rows)],
                r_s, r_r.at[int(i >= NSP // 2)], device_id=(d, t), device_id_type=MESH,
            )
            for tile, row, rows in pieces(i)
        ]

    def arrive(w):
        bulk(xin3, SIZES[w] - (w == 0), d_s, d_r.at[w]).wait_recv()
        forward(w).start()

    def gate_up(w):
        forward(w).wait_recv()
        if w == 0:
            for i in (8, 9, 10):
                copies[i].wait()
        rows = slice(2 * FIRST[w] * SLOT, 2 * (FIRST[w] + SIZES[w]) * SLOT)
        for c in range(HID // 256):
            cols = slice(c * 256, (c + 1) * 256)
            gate = jnp.dot(xin[rows, :], wg[:, cols], preferred_element_type=F32)
            up = jnp.dot(xin[rows, :], wu[:, cols], preferred_element_type=F32)
            act = jnp.minimum(gate, CLAMP_LIMIT)
            lin = jnp.clip(up, -CLAMP_LIMIT, CLAMP_LIMIT) + 1.0
            hid[0 : 2 * SIZES[w] * SLOT, cols] = (lin * act * jax.nn.sigmoid(GATE_ALPHA * act)).astype(BF)

    def down(w):
        rows = slice(2 * FIRST[w] * SLOT, 2 * (FIRST[w] + SIZES[w]) * SLOT)
        for c in range(DM // 256):
            cols = slice(c * 256, (c + 1) * 256)
            part[rows, cols] = jnp.dot(
                hid[0 : 2 * SIZES[w] * SLOT, :], wd[:, cols], preferred_element_type=F32
            ).astype(BF)
        halves(w).start()

    def finish(w):
        halves(w).wait_recv()
        own = pl.ds(wave_rows(w, t), SIZES[w] * SLOT)
        rows = slice(FIRST[w] * SLOT, (FIRST[w] + SIZES[w]) * SLOT)
        for c in range(DM // 512):
            cols = slice(c * 512, (c + 1) * 512)
            back[rows, cols] = (
                part[own, cols].astype(F32) + recv[rows, cols].astype(F32)
            ).astype(BF)
        for i in range(max(1, FIRST[w]), FIRST[w] + SIZES[w]):
            for copy in give_back(i):
                copy.start()
        if w == 0:
            ret[0:SLOT, :] = back[0:SLOT, :]

    steps = {"a": arrive, "u": gate_up, "d": down, "f": finish}
    for step in PLAN:
        steps[step[0]](int(step[1:]))

    def combine(part_of):
        rows = slice(part_of * SLOTS // 2, (part_of + 1) * SLOTS // 2)
        for c in range(8):
            cols = slice(c * 256, (c + 1) * 256)
            total = midway[:, cols]
            for k in range(2):
                total = total + jnp.dot(
                    comb[part_of, k], ret[rows, cols], preferred_element_type=F32
                )
            if part_of == 1:
                out[:, cols] = total.astype(BF)
            else:
                midway[:, cols] = total

    bulk(xin3, NSP - 1, d_s, d_r.at[0]).wait_send()
    for w in range(WAVES):
        forward(w).wait_send()
        halves(w).wait_send()
    bulk(xin3, NSP // 2 - 1, r_s, r_r.at[0]).wait_recv()
    combine(0)
    bulk(xin3, NSP // 2, r_s, r_r.at[1]).wait_recv()
    combine(1)
    bulk(xin3, NSP - 1, r_s, r_r.at[0]).wait_send()


def per_device(
    queries, keys, values, sink_logit, w_out, residual, norm_gain, w_gate, w_up, w_down,
    expert_ids, route_weight,
):
    any_spec = pl.BlockSpec(memory_space=pltpu.HBM)
    specs = [any_spec] * 13
    code = [dz * 16 + dy * 4 + dx for dz, dy, dx in ORDER]
    rows = [c * 8 + j for c in code for j in range(SLOT)]
    table = np.array(rows, np.int32)[:, None].repeat(WIN, 1)
    dma = pltpu.SemaphoreType.DMA
    return pl.pallas_call(
        body,
        out_shape=pltpu.VMEM((WIN, DM), BF),
        in_specs=specs,
        out_specs=pl.BlockSpec(memory_space=pltpu.VMEM),
        scratch_shapes=[
            pltpu.VMEM((2 * WIN, 512), BF),
            pltpu.VMEM((2, 4 * WIN, WIN), BF),
            pltpu.VMEM((2, 2, 4 * WIN, WIN), BF),
            pltpu.VMEM((2, 2, 4 * WIN, 2 * WIN), BF),
            pltpu.VMEM((2, WIN, WIN), F32),
            pltpu.VMEM((2, 4, WIN, 2 * WIN), F32),
            pltpu.VMEM((2, 4, 2, WIN, WIN), F32),
            pltpu.VMEM((2 * WIN, 512), BF),
            pltpu.VMEM((WIN, 512), BF),
            pltpu.SMEM((8,), F32),
            pltpu.VMEM((1024, DM), BF),
            pltpu.VMEM((WIN, DM), BF),
            pltpu.VMEM((1, DM), F32),
            pltpu.VMEM((DM, HID), BF),
            pltpu.VMEM((DM, HID), BF),
            pltpu.VMEM((HID, DM), BF),
            pltpu.VMEM((2, WIN), jnp.int32),
            pltpu.VMEM((2, WIN), F32),
            pltpu.VMEM((SLOTS, WIN), jnp.int32),
            pltpu.VMEM((WIN, DM), F32),
            pltpu.VMEM((WIN, DM), BF),
            pltpu.VMEM((SLOTS, WIN), BF),
            pltpu.VMEM((2, 2, WIN, SLOTS // 2), BF),
            pltpu.VMEM((SLOTS // TILE, TILE, DM), BF),
            pltpu.VMEM((2 * SLOTS // TILE, TILE, DM), BF),
            pltpu.VMEM((2 * MOST * SLOT, HID), BF),
            pltpu.VMEM((2 * SLOTS, DM), BF),
            pltpu.VMEM((SLOTS, DM), BF),
            pltpu.VMEM((SLOTS // TILE, TILE, DM), BF),
            pltpu.VMEM((SLOTS // TILE, TILE, DM), BF),
            dma((13,)),
            dma((2,)),
            dma((2,)),
            dma,
            dma,
            dma,
            dma((WAVES,)),
            dma((WAVES,)),
            dma((WAVES,)),
            dma((WAVES,)),
            dma((WAVES,)),
            dma,
            dma((2,)),
        ],
        compiler_params=pltpu.CompilerParams(
            collective_id=0, has_side_effects=True, vmem_limit_bytes=58 * 2**20
        ),
    )(
        queries, keys, values, sink_logit, w_out, residual, norm_gain.reshape(1, DM),
        w_gate[0], w_up[0], w_down[0], expert_ids.T, route_weight.T, jnp.asarray(table),
    )


def solution(mesh):
    in_specs = (
        P("sp", "tp"),
        P("sp", "tp"),
        P("sp", "tp"),
        P("tp"),
        P(),
        P(("sp", "tp"), None),
        P(),
        P("sp", None, "tp"),
        P("sp", None, "tp"),
        P("sp", "tp", None),
        P(("sp", "tp"), None),
        P(("sp", "tp"), None),
    )
    return jax.shard_map(
        per_device,
        mesh=mesh,
        in_specs=in_specs,
        out_specs=P(("sp", "tp"), None),
        check_vma=False,
    )
```

```python
import functools
import random

import jax
import jax.numpy as jnp
import numpy as np
from jax import lax
from jax.experimental import pallas as pl
from jax.experimental.pallas import tpu as pltpu
from jax.sharding import PartitionSpec as P

MESH = pl.DeviceIdType.MESH
BF = jnp.bfloat16
F32 = jnp.float32

NSP = 64
WIN = 128
DM = 2048
HID = 1024
SLOT = 6
TILE = 8
SIZES = (8, 8, 16, 16, 16)
WAVES = len(SIZES)
PLAN = (
    "a0", "u0", "a1", "d0", "u1", "f0", "a2", "d1", "a3", "u2",
    "f1", "d2", "a4", "u3", "f2", "d3", "u4", "f3", "d4", "f4",
)
FIRST = [sum(SIZES[:w]) for w in range(WAVES)]
MOST = max(SIZES)
SLOTS = NSP * SLOT
STAGES = (0, 32, 48, 64)


def pieces(i):
    at, end = i * SLOT, (i + 1) * SLOT
    while at < end:
        upto = min(end, (at // TILE + 1) * TILE)
        yield at // TILE, at % TILE, upto - at
        at = upto
CLAMP_LIMIT = 7.0
GATE_ALPHA = 1.702
EPSILON = 1e-06
NEG_BIG = -1e30
EXP_SCALE = 1.4426950408889634 / 8.0


def offsets():
    every = [(a, b, c) for a in range(4) for b in range(4) for c in range(4)]
    seen, groups = {(0, 0, 0)}, []
    for o in every:
        if o in seen:
            continue
        group = []
        for p in ((0, 1, 2), (1, 2, 0), (2, 0, 1)):
            for s in (1, -1):
                m = tuple((s * o[i]) % 4 for i in p)
                if m not in group:
                    group.append(m)
        seen |= set(group)
        groups.append(group)
    random.Random(1).shuffle(groups)
    groups.sort(key=lambda g: -sum(min(v, 4 - v) for v in g[0]))
    return [(0, 0, 0)] + [o for g in groups for o in g]


ORDER = offsets()


def shifted(me, off, sign):
    z, y, x = me // 16, (me // 4) % 4, me % 4
    dz, dy, dx = [(sign * v) % 4 for v in off]
    return ((z + dz) % 4) * 16 + ((y + dy) % 4) * 4 + (x + dx) % 4


def body(
    q_hbm, k_hbm, v_hbm, sink_hbm, wout_hbm, res_hbm, gain_hbm, wg_hbm, wu_hbm, wd_hbm, ids_hbm, rw_hbm,
    tab_hbm, out,
    q_v, kv, kmask, vmask, bias, near, peaks, att, attx, sink, wout, res, gain, wg, wu, wd, ids, rw, tab,
    midway, normed, disp, comb, xbuf3, xin3, hid, part, recv, back3, ret3,
    local_sem, halo_s, halo_r, att_s, att_r, d_s, d_r, f_s, f_r, p_s, p_r, r_s, r_r,
):
    me = lax.axis_index("sp")
    t = lax.axis_index("tp")
    other = 1 - t
    xbuf, back, ret = [b.reshape(SLOTS, DM) for b in (xbuf3, back3, ret3)]
    xin = xin3.reshape(2 * SLOTS, DM)
    right = lax.rem(me + 1, NSP)
    left = lax.rem(me + NSP - 1, NSP)

    loads = [
        (k_hbm, kv.at[0, pl.ds(WIN, 2 * WIN)]),
        (v_hbm, kv.at[1, pl.ds(WIN, 2 * WIN)]),
        (q_hbm, q_v),
        (ids_hbm, ids),
        (rw_hbm, rw),
        (wout_hbm, wout),
        (res_hbm, res),
        (gain_hbm, gain),
        (wg_hbm, wg),
        (wu_hbm, wu),
        (wd_hbm, wd),
        (tab_hbm, tab),
        (sink_hbm, sink),
    ]
    copies = [
        pltpu.make_async_copy(a, b, local_sem.at[i]) for i, (a, b) in enumerate(loads)
    ]
    for i in (0, 1, 2, 12, 3, 4, 11, 6, 7, 5, 8, 9, 10):
        copies[i].start()

    barrier = pltpu.get_barrier_semaphore()
    pl.semaphore_signal(barrier, inc=1, device_id=(left, t), device_id_type=MESH)
    pl.semaphore_signal(barrier, inc=1, device_id=(right, t), device_id_type=MESH)
    pl.semaphore_signal(barrier, inc=1, device_id=(me, other), device_id_type=MESH)
    for i in range(2, NSP - 1):
        pl.semaphore_signal(
            barrier, inc=1, device_id=(lax.rem(me + i, NSP), t), device_id_type=MESH
        )

    row = lax.broadcasted_iota(jnp.int32, (WIN, WIN), 0)
    col = lax.broadcasted_iota(jnp.int32, (WIN, WIN), 1)
    for i in (3, 4, 11):
        copies[i].wait()
    ret[...] = jnp.zeros_like(ret)
    sub = lax.broadcasted_iota(jnp.int32, (NSP, WIN), 0)
    ohs = [(sub == ids[k : k + 1, :]).astype(F32) for k in range(2)]
    before = (row < col).astype(F32).astype(BF)
    total0 = jnp.sum(ohs[0], axis=1, keepdims=True)
    slot_rows = []
    for k in range(2):
        earlier = jnp.dot(ohs[k].astype(BF), before, preferred_element_type=F32)
        if k == 1:
            earlier = earlier + total0
        rank = jnp.sum(ohs[k] * earlier, axis=0, keepdims=True)
        slot_rows.append(ids[k : k + 1, :] * SLOT + rank.astype(jnp.int32))
    offs = tab[...] >> 3
    there = (
        ((me // 16 + offs // 16) & 3) * 16
        + (((me // 4) % 4 + offs // 4) & 3) * 4
        + ((me % 4 + offs) & 3)
    )
    srow = there * SLOT + (tab[...] & 7)
    hits = [srow == slot_rows[k] for k in range(2)]
    disp[...] = (hits[0] | hits[1]).astype(F32).astype(BF)

    copies[0].wait()
    copies[1].wait()
    pl.semaphore_wait(barrier, NSP)
    to_left = pltpu.make_async_remote_copy(
        kv.at[:, pl.ds(WIN, WIN)], kv.at[:, pl.ds(3 * WIN, WIN)], halo_s.at[0], halo_r.at[0],
        device_id=(left, t), device_id_type=MESH,
    )
    to_right = pltpu.make_async_remote_copy(
        kv.at[:, pl.ds(2 * WIN, WIN)], kv.at[:, pl.ds(0, WIN)], halo_s.at[1], halo_r.at[1],
        device_id=(right, t), device_id_type=MESH,
    )
    to_left.start()
    to_right.start()

    bias[0] = jnp.where(col >= row, 0.0, NEG_BIG)
    bias[1] = jnp.where(col <= row, 0.0, NEG_BIG)

    def spread(lo, size):
        rows = slice(lo, lo + size)
        low = lax.broadcasted_iota(jnp.int32, (size, WIN), 1) < 64
        keys = kv[0, rows].astype(F32)
        keys_r = pltpu.roll(keys, 64, 1)
        vals = kv[1, rows].astype(F32)
        vals_r = pltpu.roll(vals, 64, 1)
        ones = jnp.ones_like(keys)
        for g in range(2):
            k_lo, k_hi = (keys, keys_r) if g == 0 else (keys_r, keys)
            v_lo, v_hi = (vals, vals_r) if g == 0 else (vals_r, vals)
            kmask[g, 0, rows] = jnp.where(low, k_lo, 0.0).astype(BF)
            kmask[g, 1, rows] = jnp.where(low, 0.0, k_hi).astype(BF)
            vmask[g, 0, rows, 0:WIN] = jnp.where(low, v_lo, 0.0).astype(BF)
            vmask[g, 1, rows, 0:WIN] = jnp.where(low, 0.0, v_hi).astype(BF)
            vmask[g, 0, rows, WIN:] = jnp.where(low, ones, 0.0).astype(BF)
            vmask[g, 1, rows, WIN:] = jnp.where(low, 0.0, ones).astype(BF)

    spread(WIN, 2 * WIN)
    copies[2].wait()
    copies[12].wait()

    lane_low = lax.broadcasted_iota(jnp.int32, (WIN, WIN), 1) < 64

    def scores(qp, keys):
        return lax.dot_general(
            qp, keys, (((1,), (1,)), ((), ())), preferred_element_type=F32
        )

    def own_tile(qt, _):
        base = pl.multiple_of(qt * WIN, WIN)
        cut_a = jnp.where(qt == 1, bias[0], 0.0)
        cut_b = jnp.where(qt == 0, bias[1], 0.0)
        for pair in range(4):
            g = pair // 2
            qp = q_v[pl.ds(base, WIN), pair * WIN : (pair + 1) * WIN]
            acc = None
            for side in range(2):
                s = scores(qp, kmask[g, side, WIN : 3 * WIN, :])
                s_a = s[:, 0:WIN] + cut_a
                s_b = s[:, WIN:] + cut_b
                logit = sink[2 * pair + side] * 8.0
                peak = jnp.max(jnp.maximum(s_a, s_b), axis=1, keepdims=True)
                peak = jnp.maximum(peak, logit)
                expo = jnp.concatenate(
                    [jnp.exp2((v - peak) * EXP_SCALE).astype(BF) for v in (s_a, s_b)], axis=1
                )
                o = jnp.dot(
                    expo, vmask[g, side, WIN : 3 * WIN, :], preferred_element_type=F32
                )
                acc = o if acc is None else acc + o
                peaks[qt, pair, side] = jnp.broadcast_to(peak, (WIN, WIN))
            near[qt, pair] = acc
        return 0

    lax.fori_loop(0, 2, own_tile, 0)

    to_left.wait()
    to_right.wait()
    spread(0, WIN)
    spread(3 * WIN, WIN)

    def far_tile(step, _):
        qt = lax.rem(other + step, 2)
        base = pl.multiple_of(qt * WIN, WIN)
        edge = ((me == 0) & (qt == 0)) | ((me == NSP - 1) & (qt == 1))
        cut = jnp.where(qt == 0, bias[0], bias[1]) + jnp.where(edge, NEG_BIG, 0.0)
        keys_at = pl.ds(pl.multiple_of(qt * 3 * WIN, WIN), WIN)
        for pair in range(4):
            g = pair // 2
            qp = q_v[pl.ds(base, WIN), pair * WIN : (pair + 1) * WIN]
            acc = None
            peaks_now = []
            for side in range(2):
                s = scores(qp, kmask[g, side, keys_at, :]) + cut
                peak = jnp.maximum(
                    peaks[qt, pair, side], jnp.max(s, axis=1, keepdims=True)
                )
                expo = jnp.exp2((s - peak) * EXP_SCALE).astype(BF)
                o = jnp.dot(expo, vmask[g, side, keys_at, :], preferred_element_type=F32)
                acc = o if acc is None else acc + o
                peaks_now.append(peak)
            top = jnp.where(lane_low, peaks[qt, pair, 0], peaks[qt, pair, 1])
            peak = jnp.where(lane_low, peaks_now[0], peaks_now[1])
            logit = jnp.where(lane_low, sink[2 * pair], sink[2 * pair + 1]) * 8.0
            fade = jnp.exp2((top - peak) * EXP_SCALE)
            tail = jnp.exp2((logit - peak) * EXP_SCALE)
            div = near[qt, pair, :, WIN:] * fade + acc[:, WIN:] + tail
            att[pl.ds(base, WIN), pair * WIN : (pair + 1) * WIN] = (
                (near[qt, pair, :, 0:WIN] * fade + acc[:, 0:WIN]) / div
            ).astype(BF)

        @pl.when(step == 0)
        def _():
            send_att().start()

        return 0

    def send_att():
        return pltpu.make_async_remote_copy(
            att.at[pl.ds(pl.multiple_of(other * WIN, WIN), WIN)], attx, att_s, att_r,
            device_id=(me, other), device_id_type=MESH,
        )

    lax.fori_loop(0, 2, far_tile, 0)

    for i in (5, 6, 7):
        copies[i].wait()
    mine = pl.multiple_of(t * WIN, WIN)
    w_mine = pl.multiple_of(t * 512, 512)
    w_other = pl.multiple_of(other * 512, 512)
    for c in range(8):
        cols = slice(c * 256, (c + 1) * 256)
        midway[:, cols] = jnp.dot(
            att[pl.ds(mine, WIN), :], wout[pl.ds(w_mine, 512), cols], preferred_element_type=F32
        )
    send_att().wait()

    square = jnp.zeros((WIN, WIN), F32)
    for c in range(8):
        cols = slice(c * 256, (c + 1) * 256)
        proj = midway[:, cols] + jnp.dot(
            attx[...], wout[pl.ds(w_other, 512), cols], preferred_element_type=F32
        )
        mid = res[:, cols].astype(F32) + proj.astype(BF).astype(F32)
        midway[:, cols] = mid
        sq = mid * mid
        square = square + sq[:, 0:WIN] + sq[:, WIN:]
    inv = lax.rsqrt(jnp.sum(square, axis=1, keepdims=True) * (1.0 / DM) + EPSILON)
    for c in range(8):
        cols = slice(c * 256, (c + 1) * 256)
        normed[:, cols] = (midway[:, cols] * inv * gain[:, cols]).astype(BF)

    def tiles(count):
        return count * SLOT // TILE

    def dispatch(i):
        d = shifted(me, ORDER[i], 1)
        w = max(v for v in range(WAVES) if FIRST[v] <= i)
        shift = tiles(FIRST[w]) + t * tiles(SIZES[w])
        return [
            pltpu.make_async_remote_copy(
                xbuf3.at[tile, pl.ds(row, rows)], xin3.at[tile + shift, pl.ds(row, rows)],
                d_s, d_r.at[w], device_id=(d, t), device_id_type=MESH,
            )
            for tile, row, rows in pieces(i)
        ]

    def bulk(ref, count, send_sem, recv_sem):
        rows = ref.at[pl.ds(0, count), pl.ds(0, SLOT)]
        return pltpu.make_async_remote_copy(
            rows, rows, send_sem, recv_sem, device_id=(me, other), device_id_type=MESH
        )

    for w in range(WAVES):
        rows = slice(FIRST[w] * SLOT, (FIRST[w] + SIZES[w]) * SLOT)
        for c in range(8):
            cols = slice(c * 256, (c + 1) * 256)
            xbuf[rows, cols] = jnp.dot(
                disp[rows, :], normed[:, cols], preferred_element_type=F32
            ).astype(BF)
        for i in range(max(1, FIRST[w]), FIRST[w] + SIZES[w]):
            for copy in dispatch(i):
                copy.start()
    xin[pl.ds(pl.multiple_of(t * SIZES[0] * SLOT, TILE), SLOT), :] = xbuf[0:SLOT, :]
    weight = jnp.where(hits[0], rw[0:1, :], 0.0) + jnp.where(hits[1], rw[1:2, :], 0.0)
    for stage in range(3):
        rows = slice(STAGES[stage] * SLOT, STAGES[stage + 1] * SLOT)
        size = rows.stop - rows.start
        turned = weight[rows].T
        high = turned.astype(BF)
        comb[stage, 0, :, 0:size] = high
        comb[stage, 1, :, 0:size] = (turned - high.astype(F32)).astype(BF)

    def wave_rows(w, side):
        return pl.multiple_of((2 * FIRST[w] + side * SIZES[w]) * SLOT, 8 * SLOT)

    def forward(w):
        rows = pl.ds(2 * tiles(FIRST[w]) + t * tiles(SIZES[w]), tiles(SIZES[w]))
        return pltpu.make_async_remote_copy(
            xin3.at[rows], xin3.at[rows], f_s.at[w], f_r.at[w],
            device_id=(me, other), device_id_type=MESH,
        )

    def halves(w):
        rows = pl.ds(wave_rows(w, other), SIZES[w] * SLOT)
        return pltpu.make_async_remote_copy(
            part.at[rows], recv.at[pl.ds(FIRST[w] * SLOT, SIZES[w] * SLOT)], p_s.at[w], p_r.at[w],
            device_id=(me, other), device_id_type=MESH,
        )

    def give_back(i):
        d = shifted(me, ORDER[i], -1)
        return [
            pltpu.make_async_remote_copy(
                back3.at[tile, pl.ds(row, rows)], ret3.at[tile, pl.ds(row, rows)],
                r_s, r_r.at[int(i >= STAGES[1]) + int(i >= STAGES[2])], device_id=(d, t), device_id_type=MESH,
            )
            for tile, row, rows in pieces(i)
        ]

    def arrive(w):
        bulk(xin3, SIZES[w] - (w == 0), d_s, d_r.at[w]).wait_recv()
        forward(w).start()

    def gate_up(w):
        forward(w).wait_recv()
        if w == 0:
            for i in (8, 9, 10):
                copies[i].wait()
        rows = slice(2 * FIRST[w] * SLOT, 2 * (FIRST[w] + SIZES[w]) * SLOT)
        for c in range(HID // 256):
            cols = slice(c * 256, (c + 1) * 256)
            gate = jnp.dot(xin[rows, :], wg[:, cols], preferred_element_type=F32)
            up = jnp.dot(xin[rows, :], wu[:, cols], preferred_element_type=F32)
            act = jnp.minimum(gate, CLAMP_LIMIT)
            lin = jnp.clip(up, -CLAMP_LIMIT, CLAMP_LIMIT) + 1.0
            hid[0 : 2 * SIZES[w] * SLOT, cols] = (lin * act * jax.nn.sigmoid(GATE_ALPHA * act)).astype(BF)

    def down(w):
        rows = slice(2 * FIRST[w] * SLOT, 2 * (FIRST[w] + SIZES[w]) * SLOT)
        for c in range(DM // 256):
            cols = slice(c * 256, (c + 1) * 256)
            part[rows, cols] = jnp.dot(
                hid[0 : 2 * SIZES[w] * SLOT, :], wd[:, cols], preferred_element_type=F32
            ).astype(BF)
        halves(w).start()

    def finish(w):
        halves(w).wait_recv()
        own = pl.ds(wave_rows(w, t), SIZES[w] * SLOT)
        rows = slice(FIRST[w] * SLOT, (FIRST[w] + SIZES[w]) * SLOT)
        for c in range(DM // 512):
            cols = slice(c * 512, (c + 1) * 512)
            back[rows, cols] = (
                part[own, cols].astype(F32) + recv[rows, cols].astype(F32)
            ).astype(BF)
        for i in range(max(1, FIRST[w]), FIRST[w] + SIZES[w]):
            for copy in give_back(i):
                copy.start()
        if w == 0:
            ret[0:SLOT, :] = back[0:SLOT, :]

    steps = {"a": arrive, "u": gate_up, "d": down, "f": finish}
    for step in PLAN:
        steps[step[0]](int(step[1:]))

    def combine(part_of):
        rows = slice(STAGES[part_of] * SLOT, STAGES[part_of + 1] * SLOT)
        size = rows.stop - rows.start
        for c in range(8):
            cols = slice(c * 256, (c + 1) * 256)
            total = midway[:, cols]
            for k in range(2):
                total = total + jnp.dot(
                    comb[part_of, k, :, 0:size], ret[rows, cols], preferred_element_type=F32
                )
            if part_of == 2:
                out[:, cols] = total.astype(BF)
            else:
                midway[:, cols] = total

    bulk(xin3, NSP - 1, d_s, d_r.at[0]).wait_send()
    for w in range(WAVES):
        forward(w).wait_send()
        halves(w).wait_send()
    for stage in range(3):
        count = STAGES[stage + 1] - STAGES[stage] - (stage == 0)
        bulk(xin3, count, r_s, r_r.at[stage]).wait_recv()
        combine(stage)
    bulk(xin3, NSP - 1, r_s, r_r.at[0]).wait_send()


def per_device(
    queries, keys, values, sink_logit, w_out, residual, norm_gain, w_gate, w_up, w_down,
    expert_ids, route_weight,
):
    any_spec = pl.BlockSpec(memory_space=pltpu.HBM)
    specs = [any_spec] * 13
    code = [dz * 16 + dy * 4 + dx for dz, dy, dx in ORDER]
    rows = [c * 8 + j for c in code for j in range(SLOT)]
    table = np.array(rows, np.int32)[:, None].repeat(WIN, 1)
    dma = pltpu.SemaphoreType.DMA
    return pl.pallas_call(
        body,
        out_shape=pltpu.VMEM((WIN, DM), BF),
        in_specs=specs,
        out_specs=pl.BlockSpec(memory_space=pltpu.VMEM),
        scratch_shapes=[
            pltpu.VMEM((2 * WIN, 512), BF),
            pltpu.VMEM((2, 4 * WIN, WIN), BF),
            pltpu.VMEM((2, 2, 4 * WIN, WIN), BF),
            pltpu.VMEM((2, 2, 4 * WIN, 2 * WIN), BF),
            pltpu.VMEM((2, WIN, WIN), F32),
            pltpu.VMEM((2, 4, WIN, 2 * WIN), F32),
            pltpu.VMEM((2, 4, 2, WIN, WIN), F32),
            pltpu.VMEM((2 * WIN, 512), BF),
            pltpu.VMEM((WIN, 512), BF),
            pltpu.SMEM((8,), F32),
            pltpu.VMEM((1024, DM), BF),
            pltpu.VMEM((WIN, DM), BF),
            pltpu.VMEM((1, DM), F32),
            pltpu.VMEM((DM, HID), BF),
            pltpu.VMEM((DM, HID), BF),
            pltpu.VMEM((HID, DM), BF),
            pltpu.VMEM((2, WIN), jnp.int32),
            pltpu.VMEM((2, WIN), F32),
            pltpu.VMEM((SLOTS, WIN), jnp.int32),
            pltpu.VMEM((WIN, DM), F32),
            pltpu.VMEM((WIN, DM), BF),
            pltpu.VMEM((SLOTS, WIN), BF),
            pltpu.VMEM((3, 2, WIN, SLOTS // 2), BF),
            pltpu.VMEM((SLOTS // TILE, TILE, DM), BF),
            pltpu.VMEM((2 * SLOTS // TILE, TILE, DM), BF),
            pltpu.VMEM((2 * MOST * SLOT, HID), BF),
            pltpu.VMEM((2 * SLOTS, DM), BF),
            pltpu.VMEM((SLOTS, DM), BF),
            pltpu.VMEM((SLOTS // TILE, TILE, DM), BF),
            pltpu.VMEM((SLOTS // TILE, TILE, DM), BF),
            dma((13,)),
            dma((2,)),
            dma((2,)),
            dma,
            dma,
            dma,
            dma((WAVES,)),
            dma((WAVES,)),
            dma((WAVES,)),
            dma((WAVES,)),
            dma((WAVES,)),
            dma,
            dma((3,)),
        ],
        compiler_params=pltpu.CompilerParams(
            collective_id=0, has_side_effects=True, vmem_limit_bytes=58 * 2**20
        ),
    )(
        queries, keys, values, sink_logit, w_out, residual, norm_gain.reshape(1, DM),
        w_gate[0], w_up[0], w_down[0], expert_ids.T, route_weight.T, jnp.asarray(table),
    )


def solution(mesh):
    in_specs = (
        P("sp", "tp"),
        P("sp", "tp"),
        P("sp", "tp"),
        P("tp"),
        P(),
        P(("sp", "tp"), None),
        P(),
        P("sp", None, "tp"),
        P("sp", None, "tp"),
        P("sp", "tp", None),
        P(("sp", "tp"), None),
        P(("sp", "tp"), None),
    )
    return jax.shard_map(
        per_device,
        mesh=mesh,
        in_specs=in_specs,
        out_specs=P(("sp", "tp"), None),
        check_vma=False,
    )
```
